32 devices in a mesh: sp: 8 (over z, x), tp: 4 (over y, core).
Axes of the slice: x: 2, y: 2, z: 4, core: 2. Of those that a mesh axis runs over, the one named last changes fastest.
Arguments:
- residual_in: bfloat16 [8192, 2048], P(('sp', 'tp')), may hold values from -6 to 6
- gate_outer: bfloat16 [8192, 1024], P('sp', 'tp'), may hold values from -6 to 6
- gate_inner: bfloat16 [8192, 1024], P('sp', 'tp'), may hold values from -6 to 6
- conv_input: bfloat16 [8192, 1024], P('sp', 'tp'), may hold values from -6 to 6
- conv_taps: bfloat16 [3, 1024], P(None, 'tp'), may hold values from -5 to 5
- norm_gain: bfloat16 [1024], P('tp'), may hold values from 0.099609375 to 1.8984375
- out_weight: bfloat16 [1024, 2048], P('tp'), may hold values from -0.1875 to 0.1875
- moe_gain: bfloat16 [2048], replicated, may hold values from 0.099609375 to 1.8984375
- expert_ids: int32 [8192, 2], P(('sp', 'tp')), may hold values from 0 to 7, all different within a row; in each aligned block of 256 rows (0 to 255, 256 to 511, ...) at most 128 rows name the same one
- group_prob: float32 [8192], P(('sp', 'tp')), may hold values from 0.3 to 1
- route_prob: float32 [8192, 2], P(('sp', 'tp')), may hold values from 0.1 to 1
- expert_gate: bfloat16 [8, 2048, 512], P('sp'), may hold values from -0.125 to 0.125
- expert_up: bfloat16 [8, 2048, 512], P('sp'), may hold values from -0.125 to 0.125
- expert_down: bfloat16 [8, 512, 2048], P('sp'), may hold values from -0.25 to 0.25
Outputs:
- layer_out: bfloat16 [8192, 2048], P(('sp', 'tp'))
The draws below stay inside these ranges and needn't reach their ends.
Inputs may be any that keep to these rules, and one draw needn't show every extreme that they name: `expert_ids`: each row names 2 different experts. Within the rows of one device (aligned blocks of 256 rows) no expert is named more than 128 times.
All inputs are finite; a program needn't handle non-finite values.
Results may differ from the reference program's by a relative error of at most 0.0075.
Values may be sent and summed in bfloat16 or wider, within the bound.
A program may use at most 64 MiB of HBM per device.

```python
import math
import jax
import jax.numpy as jnp
import numpy as np
from jax import lax

D = 2048
CONV = 1024
FE = 512
KW = 3
TOPK = 2
ROWS_DEV = 256
TOKENS = 8192
EXPERTS = 8
CAPACITY = 128


def draw_conv_taps(key, part):
    first, second = jax.random.split(key)
    base = jnp.clip(jax.random.normal(first, (KW, CONV), jnp.float32), -3.0, 3.0) / jnp.sqrt(jnp.float32(KW))
    levels = jnp.array([0.35, 0.7, 1.4, 2.8], jnp.float32)
    shuffled = levels[jax.random.permutation(second, 4)]
    quarter = jnp.arange(CONV, dtype=jnp.int32) * 4 // CONV
    return (base * shuffled[quarter][None, :]).astype(jnp.bfloat16)


def shard_levels(stream_key, extent, pieces, low, high):
    factor_of, own = 1.0, jax.random.fold_in(stream_key, 6)
    for position, blocks in pieces:
        steps = jnp.exp(jax.random.uniform(jax.random.fold_in(own, position), (blocks,), jnp.float32, low / len(pieces), high / len(pieces)))
        factor_of = factor_of * jnp.repeat(steps, extent[position] // blocks).reshape([-1 if axis == position else 1 for axis in range(len(extent))])
    return factor_of


def assign_block(key, own, number, rows, number_of, top, reach, slope):
    ranking = jax.random.permutation(key, number_of)
    heavy_load, common = shares(number_of, rows * top, reach, slope, True), shares(number_of, rows * top, reach, slope, False)
    places = jnp.arange(number_of)

    def named(sizes, turn):
        used = int((sizes > 0).sum())
        fixed = max(1, used // 4)
        moved = fixed + (places - fixed + turn * (used - fixed)) % max(1, number_of - fixed)
        return jnp.zeros((number_of,), jnp.int32).at[ranking[jnp.where(places < fixed, places, moved)]].set(jnp.asarray(sizes, jnp.int32))

    sizes = jnp.where(number % 4 == 0, named(heavy_load, number // 4), named(common, number - number // 4 - 1))
    mixed = jax.random.permutation(jax.random.fold_in(own, 3), number_of)
    donor, receiver = mixed[0:number_of // 2 * 2:2], mixed[1:number_of // 2 * 2:2]
    margin = jnp.minimum(sizes[donor] - 1, reach - sizes[receiver]) // 2
    margin = jnp.where((donor == ranking[0]) | (receiver == ranking[0]) | (sizes[receiver] == 0), 0, jnp.maximum(margin, 0))
    moved = jax.random.randint(jax.random.fold_in(own, 4), (number_of // 2,), 0, 1 << 20) % (margin + 1)
    sizes = sizes.at[donor].add(-moved).at[receiver].add(moved)
    items = jnp.searchsorted(jnp.cumsum(sizes), jnp.arange(rows * top), side="right").astype(jnp.int32)
    listing = items.reshape(top, rows).T
    listing = listing[jax.random.permutation(jax.random.fold_in(own, 1), rows)]
    turn = jax.random.randint(jax.random.fold_in(own, 2), (rows, 1), 0, top)
    return jnp.take_along_axis(listing, (jnp.arange(top)[None, :] + turn) % top, axis=1)


def shares(count, total, reach, slope, full):
    loads = [(1 << 20) // math.isqrt(rank ** slope) + 1 for rank in range(1, count + 1)]
    largest = reach if full else min(reach, max(-(-total // count), total * loads[0] // sum(loads)))
    least = 1 if total - largest >= count - 1 else 0
    holding, rest = [largest] + [least] * (count - 1), total - largest - least * (count - 1)
    while rest > 0:
        candidates = [i for i in range(1, count) if holding[i] < largest] or [i for i in range(1, count) if holding[i] < reach]
        pool, left = sum([loads[i] for i in candidates]), rest
        for i in candidates:
            more = min(reach - holding[i], max(1, left * loads[i] // pool), rest)
            holding[i] = holding[i] + more
            rest = rest - more
    return np.array(holding)


def normal_values(stream_key, dims, deviation, most, cuts=(), kind=jnp.bfloat16):
    values = jax.random.normal(stream_key, dims, jnp.float32) * deviation
    if len(cuts) > 0:
        values = shard_levels(stream_key, dims, cuts, -0.22, 0.18) * values
    return jnp.clip(values, min=-most, max=most).astype(kind)


def setup_inputs(seed: int = 0) -> dict:
    key_list = jax.random.split(jax.random.key(seed), 15)
    residual_in = normal_values(key_list[0], (TOKENS, D), 1.0, 6.0, ((0, 32),))
    gate_outer = normal_values(key_list[1], (TOKENS, CONV), 1.0, 6.0, ((0, 8), (1, 4)))
    gate_inner = normal_values(key_list[2], (TOKENS, CONV), 1.0, 6.0, ((0, 8), (1, 4)))
    conv_input = normal_values(key_list[3], (TOKENS, CONV), 1.0, 6.0, ((0, 8), (1, 4)))
    conv_taps = draw_conv_taps(jax.random.fold_in(key_list[14], 71), 0)
    norm_gain = jnp.clip(1.0 + 0.18 * jax.random.normal(key_list[5], (CONV,), jnp.float32), 0.099609375, 1.8984375).astype(jnp.bfloat16)
    out_weight = normal_values(key_list[6], (CONV, D), CONV ** -0.5, 0.1875, ((0, 4),))
    moe_gain = jnp.clip(1.0 + 0.18 * jax.random.normal(key_list[7], (D,), jnp.float32), 0.099609375, 1.8984375).astype(jnp.bfloat16)
    expert_ids_keys = jax.random.split(jax.random.fold_in(key_list[8], 1), TOKENS // ROWS_DEV)
    expert_ids_turns = jax.random.permutation(jax.random.fold_in(key_list[8], 3), TOKENS // ROWS_DEV)
    expert_ids = jax.vmap(lambda own, number: assign_block(jax.random.fold_in(key_list[8], 2), own, number, ROWS_DEV, EXPERTS, TOPK, CAPACITY, 2))(expert_ids_keys, expert_ids_turns).reshape((TOKENS, TOPK))
    group_prob = jnp.clip(0.3 + 0.7 * jax.random.uniform(key_list[9], (TOKENS,), jnp.float32) ** shard_levels(key_list[9], (TOKENS,), ((0, 32),), -0.2, 0.2), 0.3, 1.0)
    route_prob = jnp.clip(0.1 + 0.9 * jax.random.uniform(key_list[10], (TOKENS, TOPK), jnp.float32) ** shard_levels(key_list[10], (TOKENS, TOPK), ((0, 32),), -0.2, 0.2), 0.1, 1.0)
    expert_gate = normal_values(key_list[11], (EXPERTS, D, FE), D ** -0.5, 0.125, ((0, 8),))
    expert_up = normal_values(key_list[12], (EXPERTS, D, FE), D ** -0.5, 0.125, ((0, 8),))
    expert_down = normal_values(key_list[13], (EXPERTS, FE, D), FE ** -0.5, 0.25, ((0, 8),))
    return dict(residual_in=residual_in, gate_outer=gate_outer, gate_inner=gate_inner, conv_input=conv_input, conv_taps=conv_taps, norm_gain=norm_gain, out_weight=out_weight, moe_gain=moe_gain, expert_ids=expert_ids, group_prob=group_prob, route_prob=route_prob, expert_gate=expert_gate, expert_up=expert_up, expert_down=expert_down)


EPSILON = 1e-06

def rms_norm(values, gain):
    floats = values.astype(jnp.float32)
    factor = lax.rsqrt(lax.optimization_barrier(jnp.mean(floats * floats, axis=-1, keepdims=True)) + EPSILON)
    return floats * factor * gain.astype(jnp.float32)

def reference(residual_in, gate_outer, gate_inner, conv_input, conv_taps, norm_gain, out_weight, moe_gain, expert_ids, group_prob, route_prob, expert_gate, expert_up, expert_down):
    inner = gate_inner.astype(jnp.float32) * conv_input.astype(jnp.float32)
    padded = jnp.concatenate([jnp.zeros((KW - 1, CONV), jnp.float32), inner], axis=0)
    tap_f = conv_taps.astype(jnp.float32)
    filtered = jnp.zeros((TOKENS, CONV), jnp.float32)
    for offset in range(KW):
        filtered = filtered + tap_f[offset][None, :] * padded[offset:offset + TOKENS]
    mixed = (gate_outer.astype(jnp.float32) * filtered).astype(jnp.bfloat16)
    normed = rms_norm(mixed, norm_gain).astype(jnp.bfloat16)
    residual = (residual_in.astype(jnp.float32) + jnp.dot(normed, out_weight, preferred_element_type=jnp.float32)).astype(jnp.bfloat16)
    routed_in = rms_norm(residual, moe_gain).astype(jnp.bfloat16)
    slots = TOKENS * TOPK
    block_rows = 256
    flat_e = expert_ids.reshape(-1).astype(jnp.int32)
    order = jnp.argsort(flat_e, stable=True).astype(jnp.int32)
    sorted_e = flat_e[order]
    counts = jnp.bincount(flat_e, length=EXPERTS).astype(jnp.int32)
    padded_counts = (counts + block_rows - 1) // block_rows * block_rows
    pad_end = jnp.cumsum(padded_counts).astype(jnp.int32)
    pad_start = pad_end - padded_counts
    seg_start = (jnp.cumsum(counts) - counts).astype(jnp.int32)
    dest = pad_start[sorted_e] + jnp.arange(slots, dtype=jnp.int32) - seg_start[sorted_e]
    block_count = (slots + block_rows - 1) // block_rows + EXPERTS
    total_rows = block_count * block_rows
    buffer_slot = jnp.full((total_rows,), slots, jnp.int32).at[dest].set(order)
    block_expert = jnp.minimum(jnp.searchsorted(pad_end, jnp.arange(block_count, dtype=jnp.int32) * block_rows, side='right'), EXPERTS - 1).astype(jnp.int32)
    rows_pad = jnp.concatenate([routed_in, jnp.zeros((1, D), jnp.bfloat16)], axis=0)

    def one_block(items):
        slot_ids, expert = items
        token_row = jnp.where(slot_ids < slots, slot_ids // TOPK, TOKENS)
        block_in = rows_pad[token_row]
        gate_act = jnp.dot(block_in, expert_gate[expert], preferred_element_type=jnp.float32)
        up_act = jnp.dot(block_in, expert_up[expert], preferred_element_type=jnp.float32)
        hidden = (jax.nn.silu(gate_act) * up_act).astype(jnp.bfloat16)
        return jnp.dot(hidden, expert_down[expert], preferred_element_type=jnp.float32).astype(jnp.bfloat16)
    results = lax.map(one_block, (buffer_slot.reshape(block_count, block_rows), block_expert)).reshape(total_rows, D)
    slot_out = jnp.zeros((slots + 1, D), jnp.bfloat16).at[buffer_slot].set(results)[:slots]
    weights = group_prob[:, None] * route_prob / lax.optimization_barrier(jnp.sum(route_prob, axis=1, keepdims=True))
    expert_sum = lax.optimization_barrier(jnp.sum(slot_out.reshape(TOKENS, TOPK, D).astype(jnp.float32) * weights[:, :, None], axis=1))
    return (residual.astype(jnp.float32) + expert_sum).astype(jnp.bfloat16)
```

```python
import jax
import jax.numpy as jnp
from jax import lax
from jax.experimental import pallas as pl
from jax.experimental.pallas import tpu as pltpu
from jax.sharding import PartitionSpec as P

MESH = pl.DeviceIdType.MESH
EPSILON = 1e-06


def from_behind(shard, axis, by):
    devices = lax.axis_size(axis)
    pairs = [(i, i + by) for i in range(devices) if 0 <= i + by < devices]
    return lax.ppermute(shard, axis, pairs)


def rms_norm(values, gain):
    floats = values.astype(jnp.float32)
    factor = lax.rsqrt(jnp.mean(floats * floats, axis=-1, keepdims=True) + EPSILON)
    return floats * factor * gain.astype(jnp.float32)


GATHER_BYTES = 26 * 2**20
GAIN_ROWS = 16
HALO_ROWS = 16
PARTS = 4
COPIES = 64


def layer_kernel(
    outer_ref, inner_ref, input_ref, taps_ref, gain_ref, weight_ref, residual_ref, moe_ref, ids_ref, group_ref, route_ref,
    gate_hbm, up_hbm, down_hbm,
    out_ref,
    halo, sent, got, weights, both, down, tokens, near, far, near_line, far_in, far_line, columns,
    residual_sc, own_acc, line_out, line_in, pair_out, pair_in, hold, back_out, back_in, hidden_sc,
    send_sem, recv_sem, local_sem,
):
    sp, tp = lax.axis_index("sp"), lax.axis_index("tp")
    sp_size, tp_size = lax.axis_size("sp"), lax.axis_size("tp")
    core_me, line_me = tp % 2, (tp // 2) % 2
    core_bit = 1 - 2 * core_me
    line_bit = 2 - 4 * line_me
    lanes = [tp, tp + core_bit, tp + line_bit, tp + line_bit + core_bit]
    core, line = (sp, lanes[1]), (sp, lanes[2])
    x_peer = (sp + 1 - 2 * (sp % 2), tp)
    z_peer = (sp + 2 - 4 * ((sp // 2) % 2), tp)
    cross = ((sp + sp_size // 2) % sp_size, tp)
    after, before = ((sp + 1) % sp_size, tp), ((sp + sp_size - 1) % sp_size, tp)
    peers = [core, line, (sp, lanes[3]), x_peer, z_peer, cross, after, before]

    units = down.shape[2]
    slots, cuts = down.shape[0], down.shape[1]
    fetched = []
    for cut in range(cuts):
        first = pl.multiple_of((line_me * cuts + cut) * units, units)
        fetched += [
            pltpu.make_async_copy(gate_hbm.at[0, :, pl.ds(first, units)], both.at[0, cut, :, pl.ds(0, units)], local_sem.at[3 * cut]),
            pltpu.make_async_copy(up_hbm.at[0, :, pl.ds(first, units)], both.at[0, cut, :, pl.ds(units, units)], local_sem.at[3 * cut + 1]),
            pltpu.make_async_copy(down_hbm.at[0, pl.ds(first, units), :], down.at[0, cut], local_sem.at[3 * cut + 2]),
        ]
    for copy in fetched:
        copy.start()

    barrier = pltpu.get_barrier_semaphore()
    for peer in peers:
        pl.semaphore_signal(barrier, inc=1, device_id=peer, device_id_type=MESH)
    pl.semaphore_wait(barrier, len(peers))

    started = []

    def send(source, target, peer):
        number = len(started)
        copy = pltpu.make_async_remote_copy(
            src_ref=source, dst_ref=target, send_sem=send_sem.at[number], recv_sem=recv_sem.at[number],
            device_id=peer, device_id_type=MESH,
        )
        copy.start()
        started.append(copy)
        return copy

    full = inner_ref.shape[0]
    halos = [
        send(inner_ref.at[pl.ds(full - HALO_ROWS, HALO_ROWS)], halo.at[0], after),
        send(input_ref.at[pl.ds(full - HALO_ROWS, HALO_ROWS)], halo.at[1], after),
    ]
    weight_line = send(weight_ref, weights.at[1], line)
    weight_core = send(weight_ref, weights.at[0], core)
    for copy in fetched:
        copy.wait()
    x_both = send(both.at[0, core_me], both.at[1, core_me], x_peer)
    z_both = send(both.at[0, core_me], both.at[2, core_me], z_peer)
    x_down = send(down.at[0, core_me], down.at[1, core_me], x_peer)
    z_down = send(down.at[0, core_me], down.at[2, core_me], z_peer)

    ids = ids_ref[...]
    route = route_ref[...]
    scale = group_ref[...] * route / jnp.sum(route, axis=0, keepdims=True)
    half = sp_size // 2
    for slot in range(slots):
        side = (sp % half) ^ slot
        for table, base in ((near, (sp // half) * half), (far, (1 - sp // half) * half)):
            chosen = jnp.where(ids == base + side, scale, 0.0)
            table[slot : slot + 1, :] = jnp.sum(chosen, axis=0, keepdims=True)

    for copy in halos:
        copy.wait_recv()
    rows, width = residual_ref.shape
    taps = taps_ref[...].astype(jnp.float32)
    count = taps.shape[0]
    exchanged = []
    for step in (2, 3, 1, 0):
        block = lanes[step]
        first = pl.multiple_of(block * rows, rows)
        inner = inner_ref[pl.ds(first, rows)].astype(jnp.float32) * input_ref[pl.ds(first, rows)].astype(jnp.float32)
        back = pl.multiple_of(jnp.maximum(block * rows - HALO_ROWS, 0), HALO_ROWS)
        behind = inner_ref[pl.ds(back, HALO_ROWS)].astype(jnp.float32) * input_ref[pl.ds(back, HALO_ROWS)].astype(jnp.float32)
        outside = halo[0].astype(jnp.float32) * halo[1].astype(jnp.float32)
        outside = jnp.where(sp == 0, 0.0, outside)
        behind = jnp.where(block == 0, outside, behind)
        padded = jnp.concatenate([behind, inner], axis=0)
        filtered = jnp.zeros_like(inner)
        for offset in range(count):
            start = HALO_ROWS - (count - 1) + offset
            filtered = filtered + taps[offset][None, :] * padded[start : start + rows]
        mixed = (outer_ref[pl.ds(first, rows)].astype(jnp.float32) * filtered).astype(jnp.bfloat16)
        sent[step, :rows] = mixed
        sent[step, rows:] = jnp.broadcast_to(gain_ref[...], (GAIN_ROWS, mixed.shape[1]))
        if step > 0:
            exchanged.append(send(sent.at[step], got.at[step - 1], (sp, block)))
    near_copy = send(near, near_line, line)
    far_copy = send(far, far_in, cross)

    for copy in exchanged:
        copy.wait_recv()
    blocks = [sent.at[0], got.at[0], got.at[1], got.at[2]]
    total = jnp.zeros((rows, 1), jnp.float32)
    for block in blocks:
        values = block[:rows].astype(jnp.float32)
        total = total + jnp.sum(values * values, axis=1, keepdims=True)
    factor = lax.rsqrt(total / (tp_size * inner_ref.shape[1]) + EPSILON)

    def normed(block):
        gain = block[rows:][:1].astype(jnp.float32)
        return (block[:rows].astype(jnp.float32) * factor * gain).astype(jnp.bfloat16)

    weight_line.wait_recv()
    weight_both = send(weights.at[1], weights.at[2], core)
    weight_core.wait_recv()
    out = residual_ref[...].astype(jnp.float32)
    out = out + jnp.dot(normed(blocks[0]), weight_ref[...], preferred_element_type=jnp.float32)
    out = out + jnp.dot(normed(blocks[1]), weights[0], preferred_element_type=jnp.float32)
    out = out + jnp.dot(normed(blocks[2]), weights[1], preferred_element_type=jnp.float32)
    weight_both.wait_recv()
    out = out + jnp.dot(normed(blocks[3]), weights[2], preferred_element_type=jnp.float32)
    residual = out.astype(jnp.bfloat16)
    residual_sc[...] = residual
    floats = residual.astype(jnp.float32)
    mean = jnp.mean(floats * floats, axis=1, keepdims=True)
    routed = (floats * lax.rsqrt(mean + EPSILON) * moe_ref[...].astype(jnp.float32)).astype(jnp.bfloat16)

    piece = rows // PARTS
    batch = 2 * piece
    own_at, line_at, pair_at = (4, 5), (2, 3), (0, 1, 6, 7)
    for number, unit in enumerate(own_at):
        tokens[unit] = routed[number * batch : (number + 1) * batch]

    def own_rows(part):
        return tokens.at[own_at[part // 2], pl.ds((part % 2) * piece, piece)]

    def line_rows(part):
        return tokens.at[line_at[part // 2], pl.ds((part % 2) * piece, piece)]

    across, shared, beside = [], [], []

    def send_across(part):
        across.append(send(own_rows(part), tokens.at[pair_at[part], pl.ds(0, piece)], cross))

    def send_shared(part):
        shared.append(send(own_rows(part), line_rows(part), line))

    def relay(part):
        across[part].wait_recv()
        here = tokens.at[pair_at[part], pl.ds(0, piece)]
        beside.append(send(here, tokens.at[pair_at[part], pl.ds(piece, piece)], line))

    for part in range(PARTS):
        send_across(part)
    send_shared(0)
    send_shared(1)

    far_copy.wait_recv()
    far_relay = send(far_in, far_line, line)
    near_copy.wait_recv()

    def across_core(slot):
        return [
            send(both.at[slot, core_me], both.at[slot, core_me], core),
            send(down.at[slot, core_me], down.at[slot, core_me], core),
        ]

    x_both.wait_recv()
    x_down.wait_recv()
    diagonal_down = send(down.at[1, core_me], down.at[3, core_me], z_peer)
    z_both.wait_recv()
    diagonal_both = send(both.at[2, core_me], both.at[3, core_me], x_peer)
    z_down.wait_recv()
    cores = across_core(1) + across_core(2)

    relay(0)
    send_shared(2)
    far_relay.wait_recv()
    for slot in range(slots):
        for unit, table in ((own_at, near), (line_at, near_line)):
            column = table[slot : slot + 1, :].T
            for number in range(2):
                columns[slot, unit[number]] = column[number * batch : (number + 1) * batch]
        here, there = far_in[slot : slot + 1, :].T, far_line[slot : slot + 1, :].T
        for part in range(PARTS):
            take = slice(part * piece, (part + 1) * piece)
            columns[slot, pair_at[part], :piece] = here[take]
            columns[slot, pair_at[part], piece:] = there[take]
    relay(1)
    send_shared(3)
    diagonal_both.wait_recv()
    diagonal_down.wait_recv()
    cores += across_core(3)
    for copy in cores:
        copy.wait_recv()

    def expert_sum(unit, store):
        rows_in = tokens[unit]
        for slot in range(slots):
            scale_in = columns[slot, unit]
            for cut in range(cuts):
                act = jnp.dot(rows_in, both[slot, cut], preferred_element_type=jnp.float32)
                gated = jax.nn.silu(act[:, :units]) * act[:, units:]
                start = (slot * cuts + cut) * units
                hidden_sc[:, start : start + units] = (scale_in * gated).astype(jnp.bfloat16)
        hidden = hidden_sc[...]
        step = width // 4
        for tile in range(4):
            columns_at = pl.ds(tile * step, step)
            matrix = down[:, :, :, tile * step : (tile + 1) * step].reshape(slots * cuts * units, step)
            store(columns_at, jnp.dot(hidden, matrix, preferred_element_type=jnp.float32))

    pairs, lines, returned = [], [], []

    def pair_step(part):
        beside[part].wait_recv()

        def store(columns_at, value):
            hold[part, :, columns_at] = value[:piece]
            pair_out[part, :, columns_at] = value[piece:].astype(jnp.bfloat16)

        expert_sum(pair_at[part], store)
        pairs.append(send(pair_out.at[part], pair_in.at[part], line))

    def return_step(part):
        pairs[part].wait_recv()
        back_out[part] = (hold[part] + pair_in[part].astype(jnp.float32)).astype(jnp.bfloat16)
        returned.append(send(back_out.at[part], back_in.at[part], cross))

    def line_step(number):
        for part in (2 * number, 2 * number + 1):
            shared[part].wait_recv()

        def store(columns_at, value):
            line_out[number, :, columns_at] = value.astype(jnp.bfloat16)

        expert_sum(line_at[number], store)
        lines.append(send(line_out.at[number], line_in.at[number], line))

    def own_step(number):
        def store(columns_at, value):
            own_acc[number, :, columns_at] = value

        expert_sum(own_at[number], store)

    pair_step(0)
    pair_step(1)
    relay(2)
    return_step(0)
    line_step(0)
    return_step(1)
    line_step(1)
    relay(3)
    pair_step(2)
    own_step(0)
    pair_step(3)
    return_step(2)
    own_step(1)
    return_step(3)
    for number in range(2):
        lines[number].wait_recv()
        take = pl.ds(number * batch, batch)
        own_acc[number] += residual_sc[take].astype(jnp.float32) + line_in[number].astype(jnp.float32)
    for part in range(PARTS):
        returned[part].wait_recv()
        inside = pl.ds((part % 2) * piece, piece)
        value = own_acc[part // 2, inside] + back_in[part].astype(jnp.float32)
        out_ref[pl.ds(part * piece, piece)] = value.astype(jnp.bfloat16)
    for copy in started:
        copy.wait_send()


def half_slice(
    residual_in,
    gate_outer,
    gate_inner,
    conv_input,
    conv_taps,
    norm_gain,
    out_weight,
    moe_gain,
    expert_ids,
    group_prob,
    route_prob,
    expert_gate,
    expert_up,
    expert_down,
):
    sp, tp = lax.axis_size("sp"), lax.axis_size("tp")
    rows, width = residual_in.shape
    channels = gate_outer.shape[1]
    slots, cuts = sp // 2, 2
    units = expert_gate.shape[2] // tp
    piece = rows // PARTS
    wide = slots * cuts * units
    vmem = pl.BlockSpec(memory_space=pltpu.VMEM)
    hbm = pl.BlockSpec(memory_space=pl.ANY)
    half = lambda *shape: pltpu.VMEM(shape, jnp.bfloat16)
    single = lambda *shape: pltpu.VMEM(shape, jnp.float32)
    return pl.pallas_call(
        layer_kernel,
        in_specs=[vmem] * 11 + [hbm] * 3,
        out_specs=vmem,
        out_shape=jax.ShapeDtypeStruct((rows, width), jnp.bfloat16),
        scratch_shapes=[
            half(2, HALO_ROWS, channels),
            half(tp, rows + GAIN_ROWS, channels),
            half(tp - 1, rows + GAIN_ROWS, channels),
            half(tp - 1, *out_weight.shape),
            half(slots, cuts, width, 2 * units),
            half(slots, cuts, units, width),
            half(8, 2 * piece, width),
            single(slots, rows),
            single(slots, rows),
            single(slots, rows),
            single(slots, rows),
            single(slots, rows),
            single(slots, 8, 2 * piece, 1),
            half(rows, width),
            single(2, 2 * piece, width),
            half(2, 2 * piece, width),
            half(2, 2 * piece, width),
            half(PARTS, piece, width),
            half(PARTS, piece, width),
            single(PARTS, piece, width),
            half(PARTS, piece, width),
            half(PARTS, piece, width),
            half(2 * piece, wide),
            pltpu.SemaphoreType.DMA((COPIES,)),
            pltpu.SemaphoreType.DMA((COPIES,)),
            pltpu.SemaphoreType.DMA((6,)),
        ],
        compiler_params=pltpu.CompilerParams(
            collective_id=0, has_side_effects=True, vmem_limit_bytes=56 * 2**20
        ),
    )(
        gate_outer, gate_inner, conv_input, conv_taps, norm_gain[None], out_weight, residual_in, moe_gain[None],
        expert_ids.T, group_prob[None], route_prob.T, expert_gate, expert_up, expert_down,
    )


def exchange_slots(
    residual_in,
    gate_outer,
    gate_inner,
    conv_input,
    conv_taps,
    norm_gain,
    out_weight,
    moe_gain,
    expert_ids,
    group_prob,
    route_prob,
    expert_gate,
    expert_up,
    expert_down,
):
    seq_rows, channels = conv_input.shape
    taps_count = conv_taps.shape[0]
    inner = gate_inner.astype(jnp.float32) * conv_input.astype(jnp.float32)
    earlier = from_behind(inner[seq_rows - (taps_count - 1) :], "sp", 1)
    padded = jnp.concatenate([earlier, inner], axis=0)
    tap_f = conv_taps.astype(jnp.float32)
    filtered = jnp.zeros((seq_rows, channels), jnp.float32)
    for offset in range(taps_count):
        filtered = filtered + tap_f[offset][None, :] * padded[offset : offset + seq_rows]
    mixed_out = (gate_outer.astype(jnp.float32) * filtered).astype(jnp.bfloat16)
    gathered = lax.all_to_all(mixed_out, "tp", split_axis=0, concat_axis=1, tiled=True)
    full_weight, full_gain = (
        lax.all_gather(out_weight, "tp", axis=0, tiled=True),
        lax.all_gather(norm_gain, "tp", axis=0, tiled=True),
    )
    normed = rms_norm(gathered, full_gain).astype(jnp.bfloat16)
    projected = jnp.dot(normed, full_weight, preferred_element_type=jnp.float32)
    residual = (residual_in.astype(jnp.float32) + projected).astype(jnp.bfloat16)
    routed_in = rms_norm(residual, moe_gain).astype(jnp.bfloat16)
    tok_rows, width = routed_in.shape
    top_count = expert_ids.shape[1]
    local_count = expert_gate.shape[0]
    group_count = lax.axis_size("sp")
    experts_all = local_count * group_count
    capacity = 2 * tok_rows * top_count // experts_all
    slots = tok_rows * top_count
    flat_e = expert_ids.reshape(-1)
    one_hot = (flat_e[:, None] == jnp.arange(experts_all, dtype=jnp.int32)[None, :]).astype(
        jnp.int32
    )
    slot_rank = jnp.sum((jnp.cumsum(one_hot, axis=0) - 1) * one_hot, axis=1)
    owner_dev = flat_e // local_count
    local_slot = flat_e % local_count
    position = (local_slot * group_count + owner_dev) * capacity + slot_rank
    source_slot = (
        jnp.full((experts_all * capacity,), slots, jnp.int32)
        .at[position]
        .set(jnp.arange(slots, dtype=jnp.int32))
    )
    rows_pad = jnp.concatenate([routed_in, jnp.zeros((1, width), jnp.bfloat16)], axis=0)
    outgoing = rows_pad[source_slot // top_count].reshape(local_count, group_count, capacity, width)
    arrived = lax.all_to_all(outgoing, "sp", split_axis=1, concat_axis=1, tiled=True)
    gate_act = jnp.einsum(
        "esrd,edf->esrf", arrived, expert_gate, preferred_element_type=jnp.float32
    )
    up_act = jnp.einsum("esrd,edf->esrf", arrived, expert_up, preferred_element_type=jnp.float32)
    hidden = (jax.nn.silu(gate_act) * up_act).astype(jnp.bfloat16)
    result = jnp.einsum(
        "esrf,efd->esrd", hidden, expert_down, preferred_element_type=jnp.float32
    ).astype(jnp.bfloat16)
    returned = lax.all_to_all(result, "sp", split_axis=1, concat_axis=1, tiled=True)
    slot_out = returned.reshape(-1, width)[position].reshape(tok_rows, top_count, width)
    weights = group_prob[:, None] * route_prob / jnp.sum(route_prob, axis=1, keepdims=True)
    expert_sum = jnp.sum(slot_out.astype(jnp.float32) * weights[:, :, None], axis=1)
    return (residual.astype(jnp.float32) + expert_sum).astype(jnp.bfloat16)


def solution(mesh):
    in_specs = (
        P(("sp", "tp"), None),
        P("sp", "tp"),
        P("sp", "tp"),
        P("sp", "tp"),
        P(None, "tp"),
        P("tp"),
        P("tp", None),
        P(),
        P(("sp", "tp"), None),
        P(("sp", "tp")),
        P(("sp", "tp"), None),
        P("sp", None, None),
        P("sp", None, None),
        P("sp", None, None),
    )
    out_specs = P(("sp", "tp"), None)
    sp, tp = mesh.shape["sp"], mesh.shape["tp"]

    def body(*args):
        gate, outer = args[11], args[1]
        gathered = 3 * gate.size * gate.dtype.itemsize * sp // 4
        pairs = gate.shape[0] == 1 and sp == 8 and tp == 4
        sized = gate.shape[2] == 128 * tp and outer.shape[0] % (256 * tp) == 0
        if pairs and sized and gathered <= GATHER_BYTES:
            return half_slice(*args)
        return exchange_slots(*args)

    return jax.shard_map(body, mesh=mesh, in_specs=in_specs, out_specs=out_specs, check_vma=False)
```

```python
import jax
import jax.numpy as jnp
from jax import lax
from jax.experimental import pallas as pl
from jax.experimental.pallas import tpu as pltpu
from jax.sharding import PartitionSpec as P

MESH = pl.DeviceIdType.MESH
EPSILON = 1e-06


def from_behind(shard, axis, by):
    devices = lax.axis_size(axis)
    pairs = [(i, i + by) for i in range(devices) if 0 <= i + by < devices]
    return lax.ppermute(shard, axis, pairs)


def rms_norm(values, gain):
    floats = values.astype(jnp.float32)
    factor = lax.rsqrt(jnp.mean(floats * floats, axis=-1, keepdims=True) + EPSILON)
    return floats * factor * gain.astype(jnp.float32)


GATHER_BYTES = 26 * 2**20
GAIN_ROWS = 16
HALO_ROWS = 16
PARTS = 4
COPIES = 64


def layer_kernel(
    outer_hbm, inner_hbm, input_hbm, taps_hbm, weight_hbm, residual_hbm, ids_hbm, group_hbm, route_hbm,
    gate_hbm, up_hbm, down_hbm, gain_ref, moe_ref,
    out_ref,
    outer_ref, inner_ref, input_ref, taps_ref, weight_ref, residual_ref, ids_ref, group_ref, route_ref,
    halo, sent, got, weights, both, down, tokens, near, far, near_line, far_in, far_line, columns,
    residual_sc, own_acc, line_out, line_in, pair_out, pair_in, hold, back_out, back_in, hidden_sc,
    send_sem, recv_sem, local_sem,
):
    sp, tp = lax.axis_index("sp"), lax.axis_index("tp")
    sp_size, tp_size = lax.axis_size("sp"), lax.axis_size("tp")
    core_me, line_me = tp % 2, (tp // 2) % 2
    core_bit = 1 - 2 * core_me
    line_bit = 2 - 4 * line_me
    lanes = [tp, tp + core_bit, tp + line_bit, tp + line_bit + core_bit]
    core, line = (sp, lanes[1]), (sp, lanes[2])
    x_peer = (sp + 1 - 2 * (sp % 2), tp)
    z_peer = (sp + 2 - 4 * ((sp // 2) % 2), tp)
    cross = ((sp + sp_size // 2) % sp_size, tp)
    after, before = ((sp + 1) % sp_size, tp), ((sp + sp_size - 1) % sp_size, tp)
    peers = [core, line, (sp, lanes[3]), x_peer, z_peer, cross, after, before]

    loaded = {}
    for number, (name, source, target) in enumerate((
        ("weight", weight_hbm, weight_ref), ("inner", inner_hbm, inner_ref), ("input", input_hbm, input_ref),
        ("outer", outer_hbm, outer_ref), ("taps", taps_hbm, taps_ref), ("ids", ids_hbm, ids_ref),
        ("group", group_hbm, group_ref), ("route", route_hbm, route_ref), ("residual", residual_hbm, residual_ref),
    )):
        loaded[name] = pltpu.make_async_copy(source, target, local_sem.at[6 + number])
        loaded[name].start()

    units = down.shape[2]
    slots, cuts = down.shape[0], down.shape[1]
    fetched = []
    for cut in range(cuts):
        first = pl.multiple_of((line_me * cuts + cut) * units, units)
        fetched += [
            pltpu.make_async_copy(gate_hbm.at[0, :, pl.ds(first, units)], both.at[0, cut, :, pl.ds(0, units)], local_sem.at[3 * cut]),
            pltpu.make_async_copy(up_hbm.at[0, :, pl.ds(first, units)], both.at[0, cut, :, pl.ds(units, units)], local_sem.at[3 * cut + 1]),
            pltpu.make_async_copy(down_hbm.at[0, pl.ds(first, units), :], down.at[0, cut], local_sem.at[3 * cut + 2]),
        ]
    for copy in fetched:
        copy.start()

    barrier = pltpu.get_barrier_semaphore()
    for peer in peers:
        pl.semaphore_signal(barrier, inc=1, device_id=peer, device_id_type=MESH)
    pl.semaphore_wait(barrier, len(peers))

    started = []

    def prepare(source, target, peer):
        number = len(started)
        copy = pltpu.make_async_remote_copy(
            src_ref=source, dst_ref=target, send_sem=send_sem.at[number], recv_sem=recv_sem.at[number],
            device_id=peer, device_id_type=MESH,
        )
        started.append(copy)
        return copy

    def send(source, target, peer):
        copy = prepare(source, target, peer)
        copy.start()
        return copy

    for name in ("weight", "inner", "input"):
        loaded[name].wait()
    full = inner_ref.shape[0]
    rows, width = residual_ref.shape
    ends = (sp < 2) | (sp >= sp_size - 2)
    middle = jnp.logical_not(ends)
    halos = [
        send(inner_ref.at[pl.ds(full - HALO_ROWS, HALO_ROWS)], halo.at[0], after),
        send(input_ref.at[pl.ds(full - HALO_ROWS, HALO_ROWS)], halo.at[1], after),
    ]
    quarter = weight_ref.shape[0] // 4
    x_me = sp % 2

    def weight_rows(side, number):
        return pl.ds(pl.multiple_of((2 * side + number) * quarter, quarter), quarter)

    weight_line = [
        send(weight_ref.at[weight_rows(x_me, number)], weights.at[1, weight_rows(x_me, number)], line) for number in range(2)
    ]
    weight_core = send(weight_ref, weights.at[0], core)
    for copy in fetched:
        copy.wait()
    unit_half = units // 2

    def down_rows(slot, number):
        return down.at[slot, core_me, pl.ds(number * unit_half, unit_half)]

    x_down = [send(down_rows(0, 0), down_rows(1, 0), x_peer)]
    z_both = send(both.at[0, core_me], both.at[2, core_me], z_peer)
    z_down = send(down.at[0, core_me], down.at[2, core_me], z_peer)

    for name in ("ids", "group", "route", "outer", "taps", "residual"):
        loaded[name].wait()
    ids = ids_ref[...]
    route = route_ref[...]
    scale = group_ref[...] * route / jnp.sum(route, axis=0, keepdims=True)
    half = sp_size // 2
    for slot in range(slots):
        side = (sp % half) ^ slot
        for table, base in ((near, (sp // half) * half), (far, (1 - sp // half) * half)):
            chosen = jnp.where(ids == base + side, scale, 0.0)
            table[slot : slot + 1, :] = jnp.sum(chosen, axis=0, keepdims=True)

    for copy in halos:
        copy.wait_recv()
    taps = taps_ref[...].astype(jnp.float32)
    count = taps.shape[0]
    exchanged = []
    for step in (2, 3, 1, 0):
        block = lanes[step]
        first = pl.multiple_of(block * rows, rows)
        inner = inner_ref[pl.ds(first, rows)].astype(jnp.float32) * input_ref[pl.ds(first, rows)].astype(jnp.float32)
        back = pl.multiple_of(jnp.maximum(block * rows - HALO_ROWS, 0), HALO_ROWS)
        behind = inner_ref[pl.ds(back, HALO_ROWS)].astype(jnp.float32) * input_ref[pl.ds(back, HALO_ROWS)].astype(jnp.float32)
        outside = halo[0].astype(jnp.float32) * halo[1].astype(jnp.float32)
        outside = jnp.where(sp == 0, 0.0, outside)
        behind = jnp.where(block == 0, outside, behind)
        padded = jnp.concatenate([behind, inner], axis=0)
        filtered = jnp.zeros_like(inner)
        for offset in range(count):
            start = HALO_ROWS - (count - 1) + offset
            filtered = filtered + taps[offset][None, :] * padded[start : start + rows]
        mixed = (outer_ref[pl.ds(first, rows)].astype(jnp.float32) * filtered).astype(jnp.bfloat16)
        sent[step, :rows] = mixed
        sent[step, rows:] = jnp.broadcast_to(gain_ref[...].reshape(1, -1), (GAIN_ROWS, mixed.shape[1]))
        if step > 0:
            exchanged.append(send(sent.at[step], got.at[step - 1], (sp, block)))
    near_copy = send(near, near_line, line)
    far_copy = send(far, far_in, cross)

    piece = rows // PARTS
    batch = 2 * piece
    blocks = [sent.at[0], got.at[0], got.at[1], got.at[2]]
    matrices = [weight_ref, weights.at[0], weights.at[1], weights.at[2]]

    def gained(block, take):
        gain = block[rows:][:1].astype(jnp.float32)
        return (block[take].astype(jnp.float32) * gain).astype(jnp.bfloat16)

    def squares(block):
        values = block[:rows].astype(jnp.float32)
        return jnp.sum(values * values, axis=1, keepdims=True)

    def product(number, take):
        return jnp.dot(gained(blocks[number], take), matrices[number][...], preferred_element_type=jnp.float32)

    exchanged[2].wait_recv()
    weight_core.wait_recv()
    for number in range(2):
        take = slice(number * batch, (number + 1) * batch)
        own_acc[number] = product(0, take) + product(1, take)
    partial = squares(blocks[0]) + squares(blocks[1])

    weight_x, weight_both = [], []
    for number in range(2):
        weight_line[number].wait_recv()
        arrived = weights.at[1, weight_rows(x_me, number)]
        weight_x.append(send(arrived, arrived, x_peer))
        weight_both.append(send(arrived, weights.at[2, weight_rows(x_me, number)], core))
    x_down.append(send(down_rows(0, 1), down_rows(1, 1), x_peer))
    x_both = send(both.at[0, core_me], both.at[1, core_me], x_peer)
    x_down[0].wait_recv()
    diagonal_down = [send(down_rows(1, 0), down_rows(3, 0), z_peer)]
    for number in range(2):
        weight_x[number].wait_recv()
        arrived = weights.at[1, weight_rows(1 - x_me, number)]
        weight_both.append(send(arrived, weights.at[2, weight_rows(1 - x_me, number)], core))

    for copy in exchanged[:2]:
        copy.wait_recv()
    total = partial + squares(blocks[2]) + squares(blocks[3])
    factor = lax.rsqrt(total / (tp_size * inner_ref.shape[1]) + EPSILON)
    for copy in weight_both:
        copy.wait_recv()
    own_at, line_at, pair_at = (4, 5), (2, 3), (0, 1, 6, 7)
    for number, unit in enumerate(own_at):
        take = slice(number * batch, (number + 1) * batch)
        projected = own_acc[number] + product(2, take) + product(3, take)
        out = residual_ref[take].astype(jnp.float32) + factor[take] * projected
        residual = out.astype(jnp.bfloat16)
        residual_sc[take] = residual
        floats = residual.astype(jnp.float32)
        mean = jnp.mean(floats * floats, axis=1, keepdims=True)
        routed = floats * lax.rsqrt(mean + EPSILON) * moe_ref[...].reshape(1, -1).astype(jnp.float32)
        tokens[unit] = routed.astype(jnp.bfloat16)

    def own_rows(part):
        return tokens.at[own_at[part // 2], pl.ds((part % 2) * piece, piece)]

    def line_rows(part):
        return tokens.at[line_at[part // 2], pl.ds((part % 2) * piece, piece)]

    def pair_rows(part, second):
        return tokens.at[pair_at[part], pl.ds(second * piece, piece)]

    across = [send(own_rows(part), pair_rows(part, 0), cross) for part in range(PARTS)]
    shared = [prepare(own_rows(part), line_rows(part), line) for part in range(PARTS)]
    beside = [prepare(pair_rows(part, 0), pair_rows(part, 1), line) for part in range(PARTS)]
    for copy in shared:
        copy.start()

    def relay(parts):
        for part in parts:
            across[part].wait_recv()
            beside[part].start()

    far_copy.wait_recv()
    far_relay = send(far_in, far_line, line)
    near_copy.wait_recv()

    z_both.wait_recv()
    diagonal_both = send(both.at[2, core_me], both.at[3, core_me], x_peer)
    cores = [send(both.at[2, core_me], both.at[2, core_me], core)]
    x_down[1].wait_recv()
    diagonal_down.append(send(down_rows(1, 1), down_rows(3, 1), z_peer))
    cores.append(send(down.at[1, core_me], down.at[1, core_me], core))

    @pl.when(middle)
    def _():
        relay((0, 1))

    z_down.wait_recv()
    cores.append(send(down.at[2, core_me], down.at[2, core_me], core))

    @pl.when(middle)
    def _():
        relay((2, 3))

    far_relay.wait_recv()
    for slot in range(slots):
        for unit, table in ((own_at, near), (line_at, near_line)):
            column = table[slot : slot + 1, :].T
            for number in range(2):
                columns[slot, unit[number]] = column[number * batch : (number + 1) * batch]
        here, there = far_in[slot : slot + 1, :].T, far_line[slot : slot + 1, :].T
        for part in range(PARTS):
            take = slice(part * piece, (part + 1) * piece)
            columns[slot, pair_at[part], :piece] = here[take]
            columns[slot, pair_at[part], piece:] = there[take]

    x_both.wait_recv()
    cores.append(send(both.at[1, core_me], both.at[1, core_me], core))

    @pl.when(ends)
    def _():
        relay((0, 1, 2))

    for copy in diagonal_down:
        copy.wait_recv()
    cores.append(send(down.at[3, core_me], down.at[3, core_me], core))
    diagonal_both.wait_recv()
    cores.append(send(both.at[3, core_me], both.at[3, core_me], core))
    for copy in cores:
        copy.wait_recv()

    def expert_sum(unit, store):
        rows_in = tokens[unit]
        for slot in range(slots):
            scale_in = columns[slot, unit]
            for cut in range(cuts):
                act = jnp.dot(rows_in, both[slot, cut], preferred_element_type=jnp.float32)
                gated = jax.nn.silu(act[:, :units]) * act[:, units:]
                start = (slot * cuts + cut) * units
                hidden_sc[:, start : start + units] = (scale_in * gated).astype(jnp.bfloat16)
        hidden = hidden_sc[...]
        step = width // 4
        for tile in range(4):
            columns_at = pl.ds(tile * step, step)
            matrix = down[:, :, :, tile * step : (tile + 1) * step].reshape(slots * cuts * units, step)
            store(columns_at, jnp.dot(hidden, matrix, preferred_element_type=jnp.float32))

    pairs, lines, returned = [], [], []

    def pair_step(part):
        beside[part].wait_recv()

        def store(columns_at, value):
            hold[part, :, columns_at] = value[:piece]
            pair_out[part, :, columns_at] = value[piece:].astype(jnp.bfloat16)

        expert_sum(pair_at[part], store)
        pairs.append(send(pair_out.at[part], pair_in.at[part], line))

    def return_step(part):
        pairs[part].wait_recv()
        back_out[part] = (hold[part] + pair_in[part].astype(jnp.float32)).astype(jnp.bfloat16)
        returned.append(send(back_out.at[part], back_in.at[part], cross))

    def line_step(number):
        for part in (2 * number, 2 * number + 1):
            shared[part].wait_recv()

        def store(columns_at, value):
            for inside in range(2):
                line_out[2 * number + inside, :, columns_at] = value[inside * piece : (inside + 1) * piece].astype(jnp.bfloat16)

        expert_sum(line_at[number], store)
        for part in (2 * number, 2 * number + 1):
            lines.append(send(line_out.at[part], line_in.at[part], line))

    def own_step(number):
        def store(columns_at, value):
            own_acc[number, :, columns_at] = value

        expert_sum(own_at[number], store)

    pair_step(0)

    @pl.when(ends)
    def _():
        relay((3,))

    pair_step(1)
    own_step(0)
    return_step(0)
    pair_step(2)
    return_step(1)
    pair_step(3)
    line_step(0)
    return_step(2)
    line_step(1)
    return_step(3)
    own_step(1)
    for part in range(PARTS):
        returned[part].wait_recv()
        lines[part].wait_recv()
        inside = pl.ds((part % 2) * piece, piece)
        take = pl.ds(part * piece, piece)
        value = own_acc[part // 2, inside] + residual_sc[take].astype(jnp.float32)
        value = value + line_in[part].astype(jnp.float32) + back_in[part].astype(jnp.float32)
        out_ref[take] = value.astype(jnp.bfloat16)
    for copy in started:
        copy.wait_send()


def half_slice(
    residual_in,
    gate_outer,
    gate_inner,
    conv_input,
    conv_taps,
    norm_gain,
    out_weight,
    moe_gain,
    expert_ids,
    group_prob,
    route_prob,
    expert_gate,
    expert_up,
    expert_down,
):
    sp, tp = lax.axis_size("sp"), lax.axis_size("tp")
    rows, width = residual_in.shape
    channels = gate_outer.shape[1]
    slots, cuts = sp // 2, 2
    units = expert_gate.shape[2] // tp
    piece = rows // PARTS
    wide = slots * cuts * units
    vmem = pl.BlockSpec(memory_space=pltpu.VMEM)
    hbm = pl.BlockSpec(memory_space=pltpu.HBM)
    half = lambda *shape: pltpu.VMEM(shape, jnp.bfloat16)
    single = lambda *shape: pltpu.VMEM(shape, jnp.float32)
    return pl.pallas_call(
        layer_kernel,
        in_specs=[hbm] * 12 + [vmem] * 2,
        out_specs=vmem,
        out_shape=jax.ShapeDtypeStruct((rows, width), jnp.bfloat16),
        scratch_shapes=[
            half(*gate_outer.shape),
            half(*gate_inner.shape),
            half(*conv_input.shape),
            half(*conv_taps.shape),
            half(*out_weight.shape),
            half(*residual_in.shape),
            pltpu.VMEM(expert_ids.shape[::-1], jnp.int32),
            single(1, rows),
            single(*route_prob.shape[::-1]),
            half(2, HALO_ROWS, channels),
            half(tp, rows + GAIN_ROWS, channels),
            half(tp - 1, rows + GAIN_ROWS, channels),
            half(tp - 1, *out_weight.shape),
            half(slots, cuts, width, 2 * units),
            half(slots, cuts, units, width),
            half(8, 2 * piece, width),
            single(slots, rows),
            single(slots, rows),
            single(slots, rows),
            single(slots, rows),
            single(slots, rows),
            single(slots, 8, 2 * piece, 1),
            half(rows, width),
            single(2, 2 * piece, width),
            half(PARTS, piece, width),
            half(PARTS, piece, width),
            half(PARTS, piece, width),
            half(PARTS, piece, width),
            single(PARTS, piece, width),
            half(PARTS, piece, width),
            half(PARTS, piece, width),
            half(2 * piece, wide),
            pltpu.SemaphoreType.DMA((COPIES,)),
            pltpu.SemaphoreType.DMA((COPIES,)),
            pltpu.SemaphoreType.DMA((15,)),
        ],
        compiler_params=pltpu.CompilerParams(
            collective_id=0, has_side_effects=True, vmem_limit_bytes=58 * 2**20
        ),
    )(
        gate_outer, gate_inner, conv_input, conv_taps, out_weight, residual_in, expert_ids.T, group_prob[None],
        route_prob.T, expert_gate, expert_up, expert_down, norm_gain, moe_gain,
    )


def exchange_slots(
    residual_in,
    gate_outer,
    gate_inner,
    conv_input,
    conv_taps,
    norm_gain,
    out_weight,
    moe_gain,
    expert_ids,
    group_prob,
    route_prob,
    expert_gate,
    expert_up,
    expert_down,
):
    seq_rows, channels = conv_input.shape
    taps_count = conv_taps.shape[0]
    inner = gate_inner.astype(jnp.float32) * conv_input.astype(jnp.float32)
    earlier = from_behind(inner[seq_rows - (taps_count - 1) :], "sp", 1)
    padded = jnp.concatenate([earlier, inner], axis=0)
    tap_f = conv_taps.astype(jnp.float32)
    filtered = jnp.zeros((seq_rows, channels), jnp.float32)
    for offset in range(taps_count):
        filtered = filtered + tap_f[offset][None, :] * padded[offset : offset + seq_rows]
    mixed_out = (gate_outer.astype(jnp.float32) * filtered).astype(jnp.bfloat16)
    gathered = lax.all_to_all(mixed_out, "tp", split_axis=0, concat_axis=1, tiled=True)
    full_weight, full_gain = (
        lax.all_gather(out_weight, "tp", axis=0, tiled=True),
        lax.all_gather(norm_gain, "tp", axis=0, tiled=True),
    )
    normed = rms_norm(gathered, full_gain).astype(jnp.bfloat16)
    projected = jnp.dot(normed, full_weight, preferred_element_type=jnp.float32)
    residual = (residual_in.astype(jnp.float32) + projected).astype(jnp.bfloat16)
    routed_in = rms_norm(residual, moe_gain).astype(jnp.bfloat16)
    tok_rows, width = routed_in.shape
    top_count = expert_ids.shape[1]
    local_count = expert_gate.shape[0]
    group_count = lax.axis_size("sp")
    experts_all = local_count * group_count
    capacity = 2 * tok_rows * top_count // experts_all
    slots = tok_rows * top_count
    flat_e = expert_ids.reshape(-1)
    one_hot = (flat_e[:, None] == jnp.arange(experts_all, dtype=jnp.int32)[None, :]).astype(
        jnp.int32
    )
    slot_rank = jnp.sum((jnp.cumsum(one_hot, axis=0) - 1) * one_hot, axis=1)
    owner_dev = flat_e // local_count
    local_slot = flat_e % local_count
    position = (local_slot * group_count + owner_dev) * capacity + slot_rank
    source_slot = (
        jnp.full((experts_all * capacity,), slots, jnp.int32)
        .at[position]
        .set(jnp.arange(slots, dtype=jnp.int32))
    )
    rows_pad = jnp.concatenate([routed_in, jnp.zeros((1, width), jnp.bfloat16)], axis=0)
    outgoing = rows_pad[source_slot // top_count].reshape(local_count, group_count, capacity, width)
    arrived = lax.all_to_all(outgoing, "sp", split_axis=1, concat_axis=1, tiled=True)
    gate_act = jnp.einsum(
        "esrd,edf->esrf", arrived, expert_gate, preferred_element_type=jnp.float32
    )
    up_act = jnp.einsum("esrd,edf->esrf", arrived, expert_up, preferred_element_type=jnp.float32)
    hidden = (jax.nn.silu(gate_act) * up_act).astype(jnp.bfloat16)
    result = jnp.einsum(
        "esrf,efd->esrd", hidden, expert_down, preferred_element_type=jnp.float32
    ).astype(jnp.bfloat16)
    returned = lax.all_to_all(result, "sp", split_axis=1, concat_axis=1, tiled=True)
    slot_out = returned.reshape(-1, width)[position].reshape(tok_rows, top_count, width)
    weights = group_prob[:, None] * route_prob / jnp.sum(route_prob, axis=1, keepdims=True)
    expert_sum = jnp.sum(slot_out.astype(jnp.float32) * weights[:, :, None], axis=1)
    return (residual.astype(jnp.float32) + expert_sum).astype(jnp.bfloat16)


def solution(mesh):
    in_specs = (
        P(("sp", "tp"), None),
        P("sp", "tp"),
        P("sp", "tp"),
        P("sp", "tp"),
        P(None, "tp"),
        P("tp"),
        P("tp", None),
        P(),
        P(("sp", "tp"), None),
        P(("sp", "tp")),
        P(("sp", "tp"), None),
        P("sp", None, None),
        P("sp", None, None),
        P("sp", None, None),
    )
    out_specs = P(("sp", "tp"), None)
    sp, tp = mesh.shape["sp"], mesh.shape["tp"]

    def body(*args):
        gate, outer = args[11], args[1]
        gathered = 3 * gate.size * gate.dtype.itemsize * sp // 4
        pairs = gate.shape[0] == 1 and sp == 8 and tp == 4
        sized = gate.shape[2] == 128 * tp and outer.shape[0] % (256 * tp) == 0
        if pairs and sized and gathered <= GATHER_BYTES:
            return half_slice(*args)
        return exchange_slots(*args)

    return jax.shard_map(body, mesh=mesh, in_specs=in_specs, out_specs=out_specs, check_vma=False)
```

```python
import jax
import jax.numpy as jnp
from jax import lax
from jax.experimental import pallas as pl
from jax.experimental.pallas import tpu as pltpu
from jax.sharding import PartitionSpec as P

MESH = pl.DeviceIdType.MESH
EPSILON = 1e-06


def from_behind(shard, axis, by):
    devices = lax.axis_size(axis)
    pairs = [(i, i + by) for i in range(devices) if 0 <= i + by < devices]
    return lax.ppermute(shard, axis, pairs)


def rms_norm(values, gain):
    floats = values.astype(jnp.float32)
    factor = lax.rsqrt(jnp.mean(floats * floats, axis=-1, keepdims=True) + EPSILON)
    return floats * factor * gain.astype(jnp.float32)


GATHER_BYTES = 26 * 2**20
GAIN_ROWS = 16
HALO_ROWS = 16
PARTS = 4
COPIES = 80


def layer_kernel(
    outer_hbm, inner_hbm, input_hbm, taps_hbm, weight_hbm, residual_hbm, ids_hbm, group_hbm, route_hbm,
    gate_hbm, up_hbm, down_hbm, gain_ref, moe_ref,
    out_ref,
    outer_ref, inner_ref, input_ref, taps_ref, weight_ref, residual_ref, ids_ref, group_ref, route_ref,
    halo, sent, got, weights, both, down, tokens, near, far, near_side, far_in, far_side, columns,
    residual_sc, own_acc, line_out, line_in, pair_out, pair_in, hold, back_out, back_in, hidden_sc,
    send_sem, recv_sem, local_sem,
):
    sp, tp = lax.axis_index("sp"), lax.axis_index("tp")
    sp_size, tp_size = lax.axis_size("sp"), lax.axis_size("tp")
    core_me, line_me = tp % 2, (tp // 2) % 2
    core_bit = 1 - 2 * core_me
    line_bit = 2 - 4 * line_me
    lanes = [tp, tp + core_bit, tp + line_bit, tp + line_bit + core_bit]
    core, line = (sp, lanes[1]), (sp, lanes[2])
    x_peer = (sp + 1 - 2 * (sp % 2), tp)
    z_peer = (sp + 2 - 4 * ((sp // 2) % 2), tp)
    cross = ((sp + sp_size // 2) % sp_size, tp)
    after, before = ((sp + 1) % sp_size, tp), ((sp + sp_size - 1) % sp_size, tp)
    peers = [core, line, (sp, lanes[3]), x_peer, z_peer, cross, after, before]

    sources = dict(
        ids=(ids_hbm, ids_ref), group=(group_hbm, group_ref), route=(route_hbm, route_ref), weight=(weight_hbm, weight_ref),
        inner=(inner_hbm, inner_ref), input=(input_hbm, input_ref), outer=(outer_hbm, outer_ref), taps=(taps_hbm, taps_ref),
        residual=(residual_hbm, residual_ref),
    )
    loaded = {}
    for number, name in enumerate(sources):
        loaded[name] = pltpu.make_async_copy(*sources[name], local_sem.at[number])
        loaded[name].start()
    units = down.shape[2]
    slots, cuts = down.shape[0], down.shape[1]
    fetched = []
    for cut in range(cuts):
        first = pl.multiple_of((tp ^ cut) * units, units)
        base = len(sources) + 3 * cut
        fetched += [
            pltpu.make_async_copy(gate_hbm.at[0, :, pl.ds(first, units)], both.at[0, cut, :, pl.ds(0, units)], local_sem.at[base]),
            pltpu.make_async_copy(up_hbm.at[0, :, pl.ds(first, units)], both.at[0, cut, :, pl.ds(units, units)], local_sem.at[base + 1]),
            pltpu.make_async_copy(down_hbm.at[0, pl.ds(first, units), :], down.at[0, cut], local_sem.at[base + 2]),
        ]
    for copy in fetched:
        copy.start()

    barrier = pltpu.get_barrier_semaphore()
    for peer in peers:
        pl.semaphore_signal(barrier, inc=1, device_id=peer, device_id_type=MESH)
    for name in sources:
        loaded[name].wait()
    ids = ids_ref[...]
    route = route_ref[...]
    scale = group_ref[...] * route / jnp.sum(route, axis=0, keepdims=True)
    half = sp_size // 2
    for number, flip in enumerate((0, 2, 1, 3)):
        side = (sp % half) ^ flip
        for table, base in ((near, (sp // half) * half), (far, (1 - sp // half) * half)):
            chosen = jnp.where(ids == base + side, scale, 0.0)
            table[number : number + 1, :] = jnp.sum(chosen, axis=0, keepdims=True)
    for copy in fetched[:3]:
        copy.wait()
    pl.semaphore_wait(barrier, len(peers))

    started = []

    def prepare(source, target, peer):
        number = len(started)
        copy = pltpu.make_async_remote_copy(
            src_ref=source, dst_ref=target, send_sem=send_sem.at[number], recv_sem=recv_sem.at[number],
            device_id=peer, device_id_type=MESH,
        )
        started.append(copy)
        return copy

    def send(source, target, peer):
        copy = prepare(source, target, peer)
        copy.start()
        return copy

    full = inner_ref.shape[0]
    rows, width = residual_ref.shape
    ends = (sp < 2) | (sp >= sp_size - 2)
    middle = jnp.logical_not(ends)
    halos = [
        send(inner_ref.at[pl.ds(full - HALO_ROWS, HALO_ROWS)], halo.at[0], after),
        send(input_ref.at[pl.ds(full - HALO_ROWS, HALO_ROWS)], halo.at[1], after),
    ]
    strips = 4
    strip = weight_ref.shape[0] // (2 * strips)
    x_me = sp % 2

    def weight_rows(side, number):
        return pl.ds(pl.multiple_of((strips * side + number) * strip, strip), strip)

    weight_line = [
        send(weight_ref.at[weight_rows(x_me, number)], weights.at[1, weight_rows(x_me, number)], line) for number in range(strips)
    ]
    weight_core = send(weight_ref, weights.at[0], core)
    far_copy = send(far, far_in, cross)
    near_copy = send(near, near_side, x_peer)
    deep, wide = width // 4, units // 2

    def slices(slot, cut):
        return [both.at[slot, cut, pl.ds(n * deep, deep)] for n in range(4)] + [
            down.at[slot, cut, pl.ds(n * wide, wide)] for n in range(2)
        ]

    z_part = [send(source, target, z_peer) for source, target in zip(slices(0, 0), slices(1, 0))]
    z_core, z_line, z_both = [], [], []

    def z_arrived(number):
        z_part[number].wait_recv()
        z_line.append(send(slices(1, 0)[number], slices(1, 2)[number], line))
        z_core.append(send(slices(1, 0)[number], slices(1, 1)[number], core))

    def line_arrived(number):
        z_line[number].wait_recv()
        z_both.append(send(slices(1, 2)[number], slices(1, 3)[number], core))

    for copy in halos:
        copy.wait_recv()
    taps = taps_ref[...].astype(jnp.float32)
    count = taps.shape[0]
    exchanged = []
    for step in (2, 3, 1, 0):
        block = lanes[step]
        first = pl.multiple_of(block * rows, rows)
        inner = inner_ref[pl.ds(first, rows)].astype(jnp.float32) * input_ref[pl.ds(first, rows)].astype(jnp.float32)
        back = pl.multiple_of(jnp.maximum(block * rows - HALO_ROWS, 0), HALO_ROWS)
        behind = inner_ref[pl.ds(back, HALO_ROWS)].astype(jnp.float32) * input_ref[pl.ds(back, HALO_ROWS)].astype(jnp.float32)
        outside = halo[0].astype(jnp.float32) * halo[1].astype(jnp.float32)
        outside = jnp.where(sp == 0, 0.0, outside)
        behind = jnp.where(block == 0, outside, behind)
        padded = jnp.concatenate([behind, inner], axis=0)
        filtered = jnp.zeros_like(inner)
        for offset in range(count):
            start = HALO_ROWS - (count - 1) + offset
            filtered = filtered + taps[offset][None, :] * padded[start : start + rows]
        mixed = (outer_ref[pl.ds(first, rows)].astype(jnp.float32) * filtered).astype(jnp.bfloat16)
        sent[step, :rows] = mixed
        sent[step, rows:] = jnp.broadcast_to(gain_ref[...].reshape(1, -1), (GAIN_ROWS, mixed.shape[1]))
        if step > 0:
            exchanged.append(send(sent.at[step], got.at[step - 1], (sp, block)))

    piece = rows // PARTS
    batch = 2 * piece
    blocks = [sent.at[0], got.at[0], got.at[1], got.at[2]]
    matrices = [weight_ref, weights.at[0], weights.at[1], weights.at[2]]

    def gained(block, take):
        gain = block[rows:][:1].astype(jnp.float32)
        return (block[take].astype(jnp.float32) * gain).astype(jnp.bfloat16)

    def squares(block):
        values = block[:rows].astype(jnp.float32)
        return jnp.sum(values * values, axis=1, keepdims=True)

    def product(number, take):
        return jnp.dot(gained(blocks[number], take), matrices[number][...], preferred_element_type=jnp.float32)

    exchanged[2].wait_recv()
    weight_core.wait_recv()
    for number in range(2):
        take = slice(number * batch, (number + 1) * batch)
        own_acc[number] = product(0, take) + product(1, take)
    partial = squares(blocks[0]) + squares(blocks[1])

    weight_x, weight_both = [], []
    for number in range(strips):
        weight_line[number].wait_recv()
        arrived = weights.at[1, weight_rows(x_me, number)]
        weight_x.append(send(arrived, arrived, x_peer))
        weight_both.append(send(arrived, weights.at[2, weight_rows(x_me, number)], core))
    z_arrived(0)
    z_arrived(1)
    for number in range(strips):
        weight_x[number].wait_recv()
        arrived = weights.at[1, weight_rows(1 - x_me, number)]
        weight_both.append(send(arrived, weights.at[2, weight_rows(1 - x_me, number)], core))

    z_arrived(2)
    far_copy.wait_recv()
    far_relay = send(far_in, far_side, x_peer)
    near_copy.wait_recv()
    for copy in exchanged[:2]:
        copy.wait_recv()
    total = partial + squares(blocks[2]) + squares(blocks[3])
    factor = lax.rsqrt(total / (tp_size * inner_ref.shape[1]) + EPSILON)
    for copy in weight_both:
        copy.wait_recv()
    own_at, line_at, pair_at = (4, 5), (2, 3), (0, 1, 6, 7)
    for number, unit in enumerate(own_at):
        take = slice(number * batch, (number + 1) * batch)
        projected = own_acc[number] + product(2, take) + product(3, take)
        out = residual_ref[take].astype(jnp.float32) + factor[take] * projected
        residual = out.astype(jnp.bfloat16)
        residual_sc[take] = residual
        floats = residual.astype(jnp.float32)
        mean = jnp.mean(floats * floats, axis=1, keepdims=True)
        routed = floats * lax.rsqrt(mean + EPSILON) * moe_ref[...].reshape(1, -1).astype(jnp.float32)
        tokens[unit] = routed.astype(jnp.bfloat16)

    def own_rows(part):
        return tokens.at[own_at[part // 2], pl.ds((part % 2) * piece, piece)]

    def line_rows(part):
        return tokens.at[line_at[part // 2], pl.ds((part % 2) * piece, piece)]

    def pair_rows(part, second):
        return tokens.at[pair_at[part], pl.ds(second * piece, piece)]

    across = [send(own_rows(part), pair_rows(part, 0), cross) for part in range(PARTS)]
    shared = [send(own_rows(part), line_rows(part), x_peer) for part in range(PARTS)]
    beside = [prepare(pair_rows(part, 0), pair_rows(part, 1), x_peer) for part in range(PARTS)]

    def relay(part):
        across[part].wait_recv()
        beside[part].start()

    def only(where, action, *arguments):
        @pl.when(where)
        def _():
            for argument in arguments:
                action(argument)

    z_arrived(3)
    line_arrived(0)
    only(ends, relay, 0)
    z_arrived(4)
    line_arrived(1)
    only(ends, relay, 1)
    far_relay.wait_recv()
    for slot in range(slots):
        for unit, table, row in ((own_at, near, slot), (line_at, near_side, slots + slot)):
            column = table[row : row + 1, :].T
            for number in range(2):
                columns[slot, unit[number]] = column[number * batch : (number + 1) * batch]
        here, there = far_in[slot : slot + 1, :].T, far_side[slots + slot : slots + slot + 1, :].T
        for part in range(PARTS):
            take = slice(part * piece, (part + 1) * piece)
            columns[slot, pair_at[part], :piece] = here[take]
            columns[slot, pair_at[part], piece:] = there[take]
    line_arrived(2)
    line_arrived(3)
    only(middle, relay, 0, 1)
    z_arrived(5)
    line_arrived(4)
    line_arrived(5)
    for copy in fetched[3:]:
        copy.wait()
    for copy in z_core + z_both:
        copy.wait_recv()

    def expert_sum(unit, store):
        rows_in = tokens[unit]
        for slot in range(slots):
            scale_in = columns[slot, unit]
            for cut in range(cuts):
                act = jnp.dot(rows_in, both[slot, cut], preferred_element_type=jnp.float32)
                gated = jax.nn.silu(act[:, :units]) * act[:, units:]
                start = (slot * cuts + cut) * units
                hidden_sc[:, start : start + units] = (scale_in * gated).astype(jnp.bfloat16)
        hidden = hidden_sc[...]
        step = width // 4
        for tile in range(4):
            columns_at = pl.ds(tile * step, step)
            matrix = down[:, :, :, tile * step : (tile + 1) * step].reshape(slots * cuts * units, step)
            store(columns_at, jnp.dot(hidden, matrix, preferred_element_type=jnp.float32))

    pairs, lines, returned = [], [], []

    def pair_step(part):
        beside[part].wait_recv()

        def store(columns_at, value):
            hold[part, :, columns_at] = value[:piece]
            pair_out[part, :, columns_at] = value[piece:].astype(jnp.bfloat16)

        expert_sum(pair_at[part], store)
        pairs.append(send(pair_out.at[part], pair_in.at[part], x_peer))

    def return_step(part):
        pairs[part].wait_recv()
        back_out[part] = (hold[part] + pair_in[part].astype(jnp.float32)).astype(jnp.bfloat16)
        returned.append(send(back_out.at[part], back_in.at[part], cross))

    def line_step(number):
        for part in (2 * number, 2 * number + 1):
            shared[part].wait_recv()

        def store(columns_at, value):
            for inside in range(2):
                line_out[2 * number + inside, :, columns_at] = value[inside * piece : (inside + 1) * piece].astype(jnp.bfloat16)

        expert_sum(line_at[number], store)
        for part in (2 * number, 2 * number + 1):
            lines.append(send(line_out.at[part], line_in.at[part], x_peer))

    def own_step(number):
        def store(columns_at, value):
            own_acc[number, :, columns_at] = value

        expert_sum(own_at[number], store)

    pair_step(0)
    only(middle, relay, 2)
    pair_step(1)
    only(middle, relay, 3)
    own_step(0)
    return_step(0)
    only(ends, relay, 2)
    return_step(1)
    only(ends, relay, 3)
    pair_step(2)
    own_step(1)
    pair_step(3)
    return_step(2)
    line_step(0)
    return_step(3)
    line_step(1)
    for part in range(PARTS):
        returned[part].wait_recv()
        lines[part].wait_recv()
        inside = pl.ds((part % 2) * piece, piece)
        take = pl.ds(part * piece, piece)
        value = own_acc[part // 2, inside] + residual_sc[take].astype(jnp.float32)
        value = value + line_in[part].astype(jnp.float32) + back_in[part].astype(jnp.float32)
        out_ref[take] = value.astype(jnp.bfloat16)
    for copy in started:
        copy.wait_send()


def half_slice(
    residual_in,
    gate_outer,
    gate_inner,
    conv_input,
    conv_taps,
    norm_gain,
    out_weight,
    moe_gain,
    expert_ids,
    group_prob,
    route_prob,
    expert_gate,
    expert_up,
    expert_down,
):
    sp, tp = lax.axis_size("sp"), lax.axis_size("tp")
    rows, width = residual_in.shape
    channels = gate_outer.shape[1]
    slots, cuts = 2, tp
    units = expert_gate.shape[2] // tp
    piece = rows // PARTS
    wide = slots * cuts * units
    vmem = pl.BlockSpec(memory_space=pltpu.VMEM)
    hbm = pl.BlockSpec(memory_space=pltpu.HBM)
    half = lambda *shape: pltpu.VMEM(shape, jnp.bfloat16)
    single = lambda *shape: pltpu.VMEM(shape, jnp.float32)
    return pl.pallas_call(
        layer_kernel,
        in_specs=[hbm] * 12 + [vmem] * 2,
        out_specs=vmem,
        out_shape=jax.ShapeDtypeStruct((rows, width), jnp.bfloat16),
        scratch_shapes=[
            half(*gate_outer.shape),
            half(*gate_inner.shape),
            half(*conv_input.shape),
            half(*conv_taps.shape),
            half(*out_weight.shape),
            half(*residual_in.shape),
            pltpu.VMEM(expert_ids.shape[::-1], jnp.int32),
            single(1, rows),
            single(*route_prob.shape[::-1]),
            half(2, HALO_ROWS, channels),
            half(tp, rows + GAIN_ROWS, channels),
            half(tp - 1, rows + GAIN_ROWS, channels),
            half(tp - 1, *out_weight.shape),
            half(slots, cuts, width, 2 * units),
            half(slots, cuts, units, width),
            half(8, 2 * piece, width),
            single(2 * slots, rows),
            single(2 * slots, rows),
            single(2 * slots, rows),
            single(2 * slots, rows),
            single(2 * slots, rows),
            single(slots, 8, 2 * piece, 1),
            half(rows, width),
            single(2, 2 * piece, width),
            half(PARTS, piece, width),
            half(PARTS, piece, width),
            half(PARTS, piece, width),
            half(PARTS, piece, width),
            single(PARTS, piece, width),
            half(PARTS, piece, width),
            half(PARTS, piece, width),
            half(2 * piece, wide),
            pltpu.SemaphoreType.DMA((COPIES,)),
            pltpu.SemaphoreType.DMA((COPIES,)),
            pltpu.SemaphoreType.DMA((9 + 3 * cuts,)),
        ],
        compiler_params=pltpu.CompilerParams(
            collective_id=0, has_side_effects=True, vmem_limit_bytes=58 * 2**20
        ),
    )(
        gate_outer, gate_inner, conv_input, conv_taps, out_weight, residual_in, expert_ids.T, group_prob[None],
        route_prob.T, expert_gate, expert_up, expert_down, norm_gain, moe_gain,
    )


def exchange_slots(
    residual_in,
    gate_outer,
    gate_inner,
    conv_input,
    conv_taps,
    norm_gain,
    out_weight,
    moe_gain,
    expert_ids,
    group_prob,
    route_prob,
    expert_gate,
    expert_up,
    expert_down,
):
    seq_rows, channels = conv_input.shape
    taps_count = conv_taps.shape[0]
    inner = gate_inner.astype(jnp.float32) * conv_input.astype(jnp.float32)
    earlier = from_behind(inner[seq_rows - (taps_count - 1) :], "sp", 1)
    padded = jnp.concatenate([earlier, inner], axis=0)
    tap_f = conv_taps.astype(jnp.float32)
    filtered = jnp.zeros((seq_rows, channels), jnp.float32)
    for offset in range(taps_count):
        filtered = filtered + tap_f[offset][None, :] * padded[offset : offset + seq_rows]
    mixed_out = (gate_outer.astype(jnp.float32) * filtered).astype(jnp.bfloat16)
    gathered = lax.all_to_all(mixed_out, "tp", split_axis=0, concat_axis=1, tiled=True)
    full_weight, full_gain = (
        lax.all_gather(out_weight, "tp", axis=0, tiled=True),
        lax.all_gather(norm_gain, "tp", axis=0, tiled=True),
    )
    normed = rms_norm(gathered, full_gain).astype(jnp.bfloat16)
    projected = jnp.dot(normed, full_weight, preferred_element_type=jnp.float32)
    residual = (residual_in.astype(jnp.float32) + projected).astype(jnp.bfloat16)
    routed_in = rms_norm(residual, moe_gain).astype(jnp.bfloat16)
    tok_rows, width = routed_in.shape
    top_count = expert_ids.shape[1]
    local_count = expert_gate.shape[0]
    group_count = lax.axis_size("sp")
    experts_all = local_count * group_count
    capacity = 2 * tok_rows * top_count // experts_all
    slots = tok_rows * top_count
    flat_e = expert_ids.reshape(-1)
    one_hot = (flat_e[:, None] == jnp.arange(experts_all, dtype=jnp.int32)[None, :]).astype(
        jnp.int32
    )
    slot_rank = jnp.sum((jnp.cumsum(one_hot, axis=0) - 1) * one_hot, axis=1)
    owner_dev = flat_e // local_count
    local_slot = flat_e % local_count
    position = (local_slot * group_count + owner_dev) * capacity + slot_rank
    source_slot = (
        jnp.full((experts_all * capacity,), slots, jnp.int32)
        .at[position]
        .set(jnp.arange(slots, dtype=jnp.int32))
    )
    rows_pad = jnp.concatenate([routed_in, jnp.zeros((1, width), jnp.bfloat16)], axis=0)
    outgoing = rows_pad[source_slot // top_count].reshape(local_count, group_count, capacity, width)
    arrived = lax.all_to_all(outgoing, "sp", split_axis=1, concat_axis=1, tiled=True)
    gate_act = jnp.einsum(
        "esrd,edf->esrf", arrived, expert_gate, preferred_element_type=jnp.float32
    )
    up_act = jnp.einsum("esrd,edf->esrf", arrived, expert_up, preferred_element_type=jnp.float32)
    hidden = (jax.nn.silu(gate_act) * up_act).astype(jnp.bfloat16)
    result = jnp.einsum(
        "esrf,efd->esrd", hidden, expert_down, preferred_element_type=jnp.float32
    ).astype(jnp.bfloat16)
    returned = lax.all_to_all(result, "sp", split_axis=1, concat_axis=1, tiled=True)
    slot_out = returned.reshape(-1, width)[position].reshape(tok_rows, top_count, width)
    weights = group_prob[:, None] * route_prob / jnp.sum(route_prob, axis=1, keepdims=True)
    expert_sum = jnp.sum(slot_out.astype(jnp.float32) * weights[:, :, None], axis=1)
    return (residual.astype(jnp.float32) + expert_sum).astype(jnp.bfloat16)


def solution(mesh):
    in_specs = (
        P(("sp", "tp"), None),
        P("sp", "tp"),
        P("sp", "tp"),
        P("sp", "tp"),
        P(None, "tp"),
        P("tp"),
        P("tp", None),
        P(),
        P(("sp", "tp"), None),
        P(("sp", "tp")),
        P(("sp", "tp"), None),
        P("sp", None, None),
        P("sp", None, None),
        P("sp", None, None),
    )
    out_specs = P(("sp", "tp"), None)
    sp, tp = mesh.shape["sp"], mesh.shape["tp"]

    def body(*args):
        gate, outer = args[11], args[1]
        gathered = 3 * gate.size * gate.dtype.itemsize * sp // 4
        pairs = gate.shape[0] == 1 and sp == 8 and tp == 4
        sized = gate.shape[2] == 128 * tp and outer.shape[0] % (256 * tp) == 0
        if pairs and sized and gathered <= GATHER_BYTES:
            return half_slice(*args)
        return exchange_slots(*args)

    return jax.shard_map(body, mesh=mesh, in_specs=in_specs, out_specs=out_specs, check_vma=False)
```

```python
import jax
import jax.numpy as jnp
from jax import lax
from jax.experimental import pallas as pl
from jax.experimental.pallas import tpu as pltpu
from jax.sharding import PartitionSpec as P

MESH = pl.DeviceIdType.MESH
EPSILON = 1e-06


def from_behind(shard, axis, by):
    devices = lax.axis_size(axis)
    pairs = [(i, i + by) for i in range(devices) if 0 <= i + by < devices]
    return lax.ppermute(shard, axis, pairs)


def rms_norm(values, gain):
    floats = values.astype(jnp.float32)
    factor = lax.rsqrt(jnp.mean(floats * floats, axis=-1, keepdims=True) + EPSILON)
    return floats * factor * gain.astype(jnp.float32)


GATHER_BYTES = 26 * 2**20
GAIN_ROWS = 16
HALO_ROWS = 16
PARTS = 4
COPIES = 67


def layer_kernel(
    outer_hbm, inner_hbm, input_hbm, taps_hbm, weight_hbm, residual_hbm, ids_hbm, group_hbm, route_hbm,
    gate_hbm, up_hbm, down_hbm, gain_ref, moe_ref,
    out_hbm,
    outer_ref, inner_ref, input_ref, taps_ref, weight_ref, residual_ref, ids_ref, group_ref, route_ref,
    halo, sent, got, weights, both, down, tokens, near, far, near_side, far_in, far_side, columns,
    residual_sc, own_acc, line_out, line_in, pair_out, pair_in, hold, back_out, back_in, hidden_sc, final,
    send_sem, recv_sem, local_sem,
):
    sp, tp = lax.axis_index("sp"), lax.axis_index("tp")
    sp_size, tp_size = lax.axis_size("sp"), lax.axis_size("tp")
    core_me, line_me = tp % 2, (tp // 2) % 2
    core_bit = 1 - 2 * core_me
    line_bit = 2 - 4 * line_me
    lanes = [tp, tp + core_bit, tp + line_bit, tp + line_bit + core_bit]
    core, line = (sp, lanes[1]), (sp, lanes[2])
    x_peer = (sp + 1 - 2 * (sp % 2), tp)
    z_peer = (sp + 2 - 4 * ((sp // 2) % 2), tp)
    cross = ((sp + sp_size // 2) % sp_size, tp)
    after, before = ((sp + 1) % sp_size, tp), ((sp + sp_size - 1) % sp_size, tp)
    peers = [core, line, (sp, lanes[3]), x_peer, z_peer, cross, after, before]

    barrier = pltpu.get_barrier_semaphore()
    for peer in peers:
        pl.semaphore_signal(barrier, inc=1, device_id=peer, device_id_type=MESH)
    units = down.shape[2]
    slots, cuts = down.shape[0], down.shape[1]
    fetched = []
    for cut in range(cuts):
        first = pl.multiple_of((tp ^ cut) * units, units)
        fetched += [
            pltpu.make_async_copy(gate_hbm.at[0, :, pl.ds(first, units)], both.at[0, cut, :, pl.ds(0, units)], local_sem.at[3 * cut]),
            pltpu.make_async_copy(up_hbm.at[0, :, pl.ds(first, units)], both.at[0, cut, :, pl.ds(units, units)], local_sem.at[3 * cut + 1]),
            pltpu.make_async_copy(down_hbm.at[0, pl.ds(first, units), :], down.at[0, cut], local_sem.at[3 * cut + 2]),
        ]
    for copy in fetched[:3]:
        copy.start()
    sources = dict(
        ids=(ids_hbm, ids_ref), group=(group_hbm, group_ref), route=(route_hbm, route_ref), inner=(inner_hbm, inner_ref),
        input=(input_hbm, input_ref), outer=(outer_hbm, outer_ref), taps=(taps_hbm, taps_ref), weight=(weight_hbm, weight_ref),
        residual=(residual_hbm, residual_ref),
    )
    loaded = {}
    for number, name in enumerate(sources):
        loaded[name] = pltpu.make_async_copy(*sources[name], local_sem.at[3 * cuts + number])
        loaded[name].start()
    pl.semaphore_wait(barrier, len(peers))

    started = []

    def prepare(source, target, peer):
        number = len(started)
        copy = pltpu.make_async_remote_copy(
            src_ref=source, dst_ref=target, send_sem=send_sem.at[number], recv_sem=recv_sem.at[number],
            device_id=peer, device_id_type=MESH,
        )
        started.append(copy)
        return copy

    def send(source, target, peer):
        copy = prepare(source, target, peer)
        copy.start()
        return copy

    full = inner_ref.shape[0]
    rows, width = residual_ref.shape
    ends = (sp < 2) | (sp >= sp_size - 2)
    middle = jnp.logical_not(ends)
    halos = [
        send(inner_hbm.at[pl.ds(full - HALO_ROWS, HALO_ROWS)], halo.at[0], after),
        send(input_hbm.at[pl.ds(full - HALO_ROWS, HALO_ROWS)], halo.at[1], after),
    ]
    strips = 4
    strip = weight_ref.shape[0] // (2 * strips)
    x_me = sp % 2

    def weight_rows(side, number):
        return pl.ds(pl.multiple_of((strips * side + number) * strip, strip), strip)

    weight_line = [
        send(weight_hbm.at[weight_rows(x_me, number)], weights.at[1, weight_rows(x_me, number)], line) for number in range(strips)
    ]
    weight_core = send(weight_hbm, weights.at[0], core)
    for name in ("ids", "group", "route"):
        loaded[name].wait()
    ids = ids_ref[...]
    route = route_ref[...]
    scale = group_ref[...] * route / jnp.sum(route, axis=0, keepdims=True)
    half = sp_size // 2
    for number, flip in enumerate((0, 2, 1, 3)):
        side = (sp % half) ^ flip
        for table, base in ((near, (sp // half) * half), (far, (1 - sp // half) * half)):
            chosen = jnp.where(ids == base + side, scale, 0.0)
            table[number : number + 1, :] = jnp.sum(chosen, axis=0, keepdims=True)
    far_copy = send(far, far_in, cross)
    near_copy = send(near, near_side, x_peer)
    deep, wide = width // 4, units // 4

    def slices(slot, cut):
        return [both.at[slot, cut, pl.ds(n * deep, deep)] for n in range(4)] + [
            down.at[slot, cut, pl.ds(n * wide, wide)] for n in range(4)
        ]

    for copy in fetched[:3]:
        copy.wait()
    z_part = [prepare(source, target, z_peer) for source, target in zip(slices(0, 0), slices(1, 0))]

    def only(where, action, *arguments):
        @pl.when(where)
        def _():
            for argument in arguments:
                action(argument)

    for copy in z_part[:4]:
        copy.start()
    only(middle, lambda number: z_part[number].start(), 4, 5, 6, 7)
    for copy in fetched[3:]:
        copy.start()
    z_core, z_line, z_both = [], [], []

    def beyond(cut, target, number, sends):
        pair = pl.ds((number // 2) * 2 * deep, 2 * deep)
        if number in (1, 3):
            sends.append(send(both.at[1, cut, pair], both.at[1, target, pair], core))
        if number == 7:
            sends.append(send(down.at[1, cut], down.at[1, target], core))

    def z_arrived(number):
        z_part[number].wait_recv()
        z_line.append(send(slices(1, 0)[number], slices(1, 2)[number], line))
        beyond(0, 1, number, z_core)

    def line_arrived(number):
        z_line[number].wait_recv()
        beyond(2, 3, number, z_both)

    for name in ("inner", "input", "outer", "taps"):
        loaded[name].wait()

    for copy in halos:
        copy.wait_recv()
    taps = taps_ref[...].astype(jnp.float32)
    count = taps.shape[0]
    exchanged = []
    for step in (2, 3, 1, 0):
        block = lanes[step]
        first = pl.multiple_of(block * rows, rows)
        inner = inner_ref[pl.ds(first, rows)].astype(jnp.float32) * input_ref[pl.ds(first, rows)].astype(jnp.float32)
        back = pl.multiple_of(jnp.maximum(block * rows - HALO_ROWS, 0), HALO_ROWS)
        behind = inner_ref[pl.ds(back, HALO_ROWS)].astype(jnp.float32) * input_ref[pl.ds(back, HALO_ROWS)].astype(jnp.float32)
        outside = halo[0].astype(jnp.float32) * halo[1].astype(jnp.float32)
        outside = jnp.where(sp == 0, 0.0, outside)
        behind = jnp.where(block == 0, outside, behind)
        padded = jnp.concatenate([behind, inner], axis=0)
        filtered = jnp.zeros_like(inner)
        for offset in range(count):
            start = HALO_ROWS - (count - 1) + offset
            filtered = filtered + taps[offset][None, :] * padded[start : start + rows]
        mixed = (outer_ref[pl.ds(first, rows)].astype(jnp.float32) * filtered).astype(jnp.bfloat16)
        sent[step, :rows] = mixed
        sent[step, rows:] = jnp.broadcast_to(gain_ref[...].reshape(1, -1), (GAIN_ROWS, mixed.shape[1]))
        if step > 0:
            exchanged.append(send(sent.at[step], got.at[step - 1], (sp, block)))

    piece = rows // PARTS
    batch = 2 * piece
    blocks = [sent.at[0], got.at[0], got.at[1], got.at[2]]
    matrices = [weight_ref, weights.at[0], weights.at[1], weights.at[2]]

    def gained(block, take):
        gain = block[rows:][:1].astype(jnp.float32)
        return (block[take].astype(jnp.float32) * gain).astype(jnp.bfloat16)

    def squares(block):
        values = block[:rows].astype(jnp.float32)
        return jnp.sum(values * values, axis=1, keepdims=True)

    def product(number, take):
        return jnp.dot(gained(blocks[number], take), matrices[number][...], preferred_element_type=jnp.float32)

    exchanged[2].wait_recv()
    weight_core.wait_recv()
    loaded["weight"].wait()
    loaded["residual"].wait()
    for number in range(2):
        take = slice(number * batch, (number + 1) * batch)
        own_acc[number] = product(0, take) + product(1, take)
    partial = squares(blocks[0]) + squares(blocks[1])

    weight_x, weight_both = [], []

    def weight_pair(side, number):
        if number % 2 == 1:
            rows_at = pl.ds(pl.multiple_of((strips * side + number - 1) * strip, 2 * strip), 2 * strip)
            weight_both.append(send(weights.at[1, rows_at], weights.at[2, rows_at], core))

    for number in range(strips):
        weight_line[number].wait_recv()
        arrived = weights.at[1, weight_rows(x_me, number)]
        weight_x.append(send(arrived, arrived, x_peer))
        weight_pair(x_me, number)
    z_arrived(0)
    z_arrived(1)
    for number in range(strips):
        weight_x[number].wait_recv()
        weight_pair(1 - x_me, number)
    far_copy.wait_recv()
    far_relay = send(far_in, far_side, x_peer)
    near_copy.wait_recv()
    for copy in exchanged[:2]:
        copy.wait_recv()
    total = partial + squares(blocks[2]) + squares(blocks[3])
    factor = lax.rsqrt(total / (tp_size * inner_ref.shape[1]) + EPSILON)
    for copy in weight_both:
        copy.wait_recv()
    own_at, line_at, pair_at = (4, 5), (2, 3), (0, 1, 6, 7)
    def own_rows(part):
        return tokens.at[own_at[part // 2], pl.ds((part % 2) * piece, piece)]

    def line_rows(part):
        return tokens.at[line_at[part // 2], pl.ds((part % 2) * piece, piece)]

    def pair_rows(part, second):
        return tokens.at[pair_at[part], pl.ds(second * piece, piece)]

    across, shared = [], []
    for number, unit in enumerate(own_at):
        take = slice(number * batch, (number + 1) * batch)
        projected = own_acc[number] + product(2, take) + product(3, take)
        out = residual_ref[take].astype(jnp.float32) + factor[take] * projected
        residual = out.astype(jnp.bfloat16)
        residual_sc[take] = residual
        floats = residual.astype(jnp.float32)
        mean = jnp.mean(floats * floats, axis=1, keepdims=True)
        routed = floats * lax.rsqrt(mean + EPSILON) * moe_ref[...].reshape(1, -1).astype(jnp.float32)
        tokens[unit] = routed.astype(jnp.bfloat16)
        for part in (2 * number, 2 * number + 1):
            across.append(send(own_rows(part), pair_rows(part, 0), cross))
            shared.append(send(own_rows(part), line_rows(part), x_peer))
        if number == 0:
            only(ends, lambda number: z_part[number].start(), 4, 5, 6, 7)

    beside = [prepare(pair_rows(part, 0), pair_rows(part, 1), x_peer) for part in range(PARTS)]

    def relay(part):
        across[part].wait_recv()
        beside[part].start()

    z_arrived(2)
    line_arrived(0)
    z_arrived(3)
    line_arrived(1)
    only(middle, relay, 0, 1)
    z_arrived(4)
    z_arrived(5)
    line_arrived(2)
    only(ends, relay, 0, 1)
    far_relay.wait_recv()
    for slot in range(slots):
        for unit, table, row in ((own_at, near, slot), (line_at, near_side, slots + slot)):
            column = table[row : row + 1, :].T
            for number in range(2):
                columns[slot, unit[number]] = column[number * batch : (number + 1) * batch]
        here, there = far_in[slot : slot + 1, :].T, far_side[slots + slot : slots + slot + 1, :].T
        for part in range(PARTS):
            take = slice(part * piece, (part + 1) * piece)
            columns[slot, pair_at[part], :piece] = here[take]
            columns[slot, pair_at[part], piece:] = there[take]
    z_arrived(6)
    z_arrived(7)
    line_arrived(3)
    for number in range(4, 8):
        line_arrived(number)
    for copy in fetched[3:]:
        copy.wait()
    for copy in z_core + z_both:
        copy.wait_recv()

    def expert_sum(unit, store):
        rows_in = tokens[unit]
        for slot in range(slots):
            scale_in = columns[slot, unit]
            for cut in range(cuts):
                act = jnp.dot(rows_in, both[slot, cut], preferred_element_type=jnp.float32)
                gated = jax.nn.silu(act[:, :units]) * act[:, units:]
                start = (slot * cuts + cut) * units
                hidden_sc[:, start : start + units] = (scale_in * gated).astype(jnp.bfloat16)
        hidden = hidden_sc[...]
        step = width // 4
        for tile in range(4):
            columns_at = pl.ds(tile * step, step)
            matrix = down[:, :, :, tile * step : (tile + 1) * step].reshape(slots * cuts * units, step)
            store(columns_at, jnp.dot(hidden, matrix, preferred_element_type=jnp.float32))

    pairs, lines, returned = [], [], []

    def pair_step(part):
        beside[part].wait_recv()

        def store(columns_at, value):
            hold[part, :, columns_at] = value[:piece]
            pair_out[part, :, columns_at] = value[piece:].astype(jnp.bfloat16)

        expert_sum(pair_at[part], store)
        pairs.append(send(pair_out.at[part], pair_in.at[part], x_peer))

    def return_step(part):
        pairs[part].wait_recv()
        back_out[part] = (hold[part] + pair_in[part].astype(jnp.float32)).astype(jnp.bfloat16)
        returned.append(send(back_out.at[part], back_in.at[part], cross))

    def line_step(number):
        for part in (2 * number, 2 * number + 1):
            shared[part].wait_recv()

        def store(columns_at, value):
            for inside in range(2):
                line_out[2 * number + inside, :, columns_at] = value[inside * piece : (inside + 1) * piece].astype(jnp.bfloat16)

        expert_sum(line_at[number], store)
        for part in (2 * number, 2 * number + 1):
            lines.append(send(line_out.at[part], line_in.at[part], x_peer))

    def own_step(number):
        def store(columns_at, value):
            own_acc[number, :, columns_at] = value

        expert_sum(own_at[number], store)

    pair_step(0)
    only(middle, relay, 2)
    pair_step(1)
    only(middle, relay, 3)
    own_step(0)
    only(ends, relay, 2, 3)
    return_step(0)
    return_step(1)
    pair_step(2)
    own_step(1)
    pair_step(3)
    return_step(2)
    line_step(0)
    return_step(3)
    line_step(1)
    late = pairs + lines + returned
    for copy in started:
        if all(copy is not other for other in late):
            copy.wait_send()
    written = []
    for part in range(PARTS):
        returned[part].wait_recv()
        lines[part].wait_recv()
        inside = pl.ds((part % 2) * piece, piece)
        take = pl.ds(part * piece, piece)
        value = own_acc[part // 2, inside] + residual_sc[take].astype(jnp.float32)
        value = value + line_in[part].astype(jnp.float32) + back_in[part].astype(jnp.float32)
        final[part] = value.astype(jnp.bfloat16)
        written.append(pltpu.make_async_copy(final.at[part], out_hbm.at[take], local_sem.at[part]))
        written[part].start()
    for copy in late:
        copy.wait_send()
    for copy in written:
        copy.wait()


def half_slice(
    residual_in,
    gate_outer,
    gate_inner,
    conv_input,
    conv_taps,
    norm_gain,
    out_weight,
    moe_gain,
    expert_ids,
    group_prob,
    route_prob,
    expert_gate,
    expert_up,
    expert_down,
):
    sp, tp = lax.axis_size("sp"), lax.axis_size("tp")
    rows, width = residual_in.shape
    channels = gate_outer.shape[1]
    slots, cuts = 2, tp
    units = expert_gate.shape[2] // tp
    piece = rows // PARTS
    wide = slots * cuts * units
    vmem = pl.BlockSpec(memory_space=pltpu.VMEM)
    hbm = pl.BlockSpec(memory_space=pltpu.HBM)
    half = lambda *shape: pltpu.VMEM(shape, jnp.bfloat16)
    single = lambda *shape: pltpu.VMEM(shape, jnp.float32)
    return pl.pallas_call(
        layer_kernel,
        in_specs=[hbm] * 12 + [vmem] * 2,
        out_specs=hbm,
        out_shape=jax.ShapeDtypeStruct((rows, width), jnp.bfloat16),
        scratch_shapes=[
            half(*gate_outer.shape),
            half(*gate_inner.shape),
            half(*conv_input.shape),
            half(*conv_taps.shape),
            half(*out_weight.shape),
            half(*residual_in.shape),
            pltpu.VMEM(expert_ids.shape[::-1], jnp.int32),
            single(1, rows),
            single(*route_prob.shape[::-1]),
            half(2, HALO_ROWS, channels),
            half(tp, rows + GAIN_ROWS, channels),
            half(tp - 1, rows + GAIN_ROWS, channels),
            half(tp - 1, *out_weight.shape),
            half(slots, cuts, width, 2 * units),
            half(slots, cuts, units, width),
            half(8, 2 * piece, width),
            single(2 * slots, rows),
            single(2 * slots, rows),
            single(2 * slots, rows),
            single(2 * slots, rows),
            single(2 * slots, rows),
            single(slots, 8, 2 * piece, 1),
            half(rows, width),
            single(2, 2 * piece, width),
            half(PARTS, piece, width),
            half(PARTS, piece, width),
            half(PARTS, piece, width),
            half(PARTS, piece, width),
            single(PARTS, piece, width),
            half(PARTS, piece, width),
            half(PARTS, piece, width),
            half(2 * piece, wide),
            half(PARTS, piece, width),
            pltpu.SemaphoreType.DMA((COPIES,)),
            pltpu.SemaphoreType.DMA((COPIES,)),
            pltpu.SemaphoreType.DMA((9 + 3 * cuts,)),
        ],
        compiler_params=pltpu.CompilerParams(
            collective_id=0, has_side_effects=True, vmem_limit_bytes=58 * 2**20
        ),
    )(
        gate_outer, gate_inner, conv_input, conv_taps, out_weight, residual_in, expert_ids.T, group_prob[None],
        route_prob.T, expert_gate, expert_up, expert_down, norm_gain, moe_gain,
    )


def exchange_slots(
    residual_in,
    gate_outer,
    gate_inner,
    conv_input,
    conv_taps,
    norm_gain,
    out_weight,
    moe_gain,
    expert_ids,
    group_prob,
    route_prob,
    expert_gate,
    expert_up,
    expert_down,
):
    seq_rows, channels = conv_input.shape
    taps_count = conv_taps.shape[0]
    inner = gate_inner.astype(jnp.float32) * conv_input.astype(jnp.float32)
    earlier = from_behind(inner[seq_rows - (taps_count - 1) :], "sp", 1)
    padded = jnp.concatenate([earlier, inner], axis=0)
    tap_f = conv_taps.astype(jnp.float32)
    filtered = jnp.zeros((seq_rows, channels), jnp.float32)
    for offset in range(taps_count):
        filtered = filtered + tap_f[offset][None, :] * padded[offset : offset + seq_rows]
    mixed_out = (gate_outer.astype(jnp.float32) * filtered).astype(jnp.bfloat16)
    gathered = lax.all_to_all(mixed_out, "tp", split_axis=0, concat_axis=1, tiled=True)
    full_weight, full_gain = (
        lax.all_gather(out_weight, "tp", axis=0, tiled=True),
        lax.all_gather(norm_gain, "tp", axis=0, tiled=True),
    )
    normed = rms_norm(gathered, full_gain).astype(jnp.bfloat16)
    projected = jnp.dot(normed, full_weight, preferred_element_type=jnp.float32)
    residual = (residual_in.astype(jnp.float32) + projected).astype(jnp.bfloat16)
    routed_in = rms_norm(residual, moe_gain).astype(jnp.bfloat16)
    tok_rows, width = routed_in.shape
    top_count = expert_ids.shape[1]
    local_count = expert_gate.shape[0]
    group_count = lax.axis_size("sp")
    experts_all = local_count * group_count
    capacity = 2 * tok_rows * top_count // experts_all
    slots = tok_rows * top_count
    flat_e = expert_ids.reshape(-1)
    one_hot = (flat_e[:, None] == jnp.arange(experts_all, dtype=jnp.int32)[None, :]).astype(
        jnp.int32
    )
    slot_rank = jnp.sum((jnp.cumsum(one_hot, axis=0) - 1) * one_hot, axis=1)
    owner_dev = flat_e // local_count
    local_slot = flat_e % local_count
    position = (local_slot * group_count + owner_dev) * capacity + slot_rank
    source_slot = (
        jnp.full((experts_all * capacity,), slots, jnp.int32)
        .at[position]
        .set(jnp.arange(slots, dtype=jnp.int32))
    )
    rows_pad = jnp.concatenate([routed_in, jnp.zeros((1, width), jnp.bfloat16)], axis=0)
    outgoing = rows_pad[source_slot // top_count].reshape(local_count, group_count, capacity, width)
    arrived = lax.all_to_all(outgoing, "sp", split_axis=1, concat_axis=1, tiled=True)
    gate_act = jnp.einsum(
        "esrd,edf->esrf", arrived, expert_gate, preferred_element_type=jnp.float32
    )
    up_act = jnp.einsum("esrd,edf->esrf", arrived, expert_up, preferred_element_type=jnp.float32)
    hidden = (jax.nn.silu(gate_act) * up_act).astype(jnp.bfloat16)
    result = jnp.einsum(
        "esrf,efd->esrd", hidden, expert_down, preferred_element_type=jnp.float32
    ).astype(jnp.bfloat16)
    returned = lax.all_to_all(result, "sp", split_axis=1, concat_axis=1, tiled=True)
    slot_out = returned.reshape(-1, width)[position].reshape(tok_rows, top_count, width)
    weights = group_prob[:, None] * route_prob / jnp.sum(route_prob, axis=1, keepdims=True)
    expert_sum = jnp.sum(slot_out.astype(jnp.float32) * weights[:, :, None], axis=1)
    return (residual.astype(jnp.float32) + expert_sum).astype(jnp.bfloat16)


def solution(mesh):
    in_specs = (
        P(("sp", "tp"), None),
        P("sp", "tp"),
        P("sp", "tp"),
        P("sp", "tp"),
        P(None, "tp"),
        P("tp"),
        P("tp", None),
        P(),
        P(("sp", "tp"), None),
        P(("sp", "tp")),
        P(("sp", "tp"), None),
        P("sp", None, None),
        P("sp", None, None),
        P("sp", None, None),
    )
    out_specs = P(("sp", "tp"), None)
    sp, tp = mesh.shape["sp"], mesh.shape["tp"]

    def body(*args):
        gate, outer = args[11], args[1]
        gathered = 3 * gate.size * gate.dtype.itemsize * sp // 4
        pairs = gate.shape[0] == 1 and sp == 8 and tp == 4
        sized = gate.shape[2] == 128 * tp and outer.shape[0] % (256 * tp) == 0
        if pairs and sized and gathered <= GATHER_BYTES:
            return half_slice(*args)
        return exchange_slots(*args)

    return jax.shard_map(body, mesh=mesh, in_specs=in_specs, out_specs=out_specs, check_vma=False)
```

```python
import jax
import jax.numpy as jnp
from jax import lax
from jax.experimental import pallas as pl
from jax.experimental.pallas import tpu as pltpu
from jax.sharding import PartitionSpec as P

MESH = pl.DeviceIdType.MESH
EPSILON = 1e-06


def from_behind(shard, axis, by):
    devices = lax.axis_size(axis)
    pairs = [(i, i + by) for i in range(devices) if 0 <= i + by < devices]
    return lax.ppermute(shard, axis, pairs)


def rms_norm(values, gain):
    floats = values.astype(jnp.float32)
    factor = lax.rsqrt(jnp.mean(floats * floats, axis=-1, keepdims=True) + EPSILON)
    return floats * factor * gain.astype(jnp.float32)


GATHER_BYTES = 26 * 2**20
GAIN_ROWS = 16
HALO_ROWS = 16
PARTS = 4
COPIES = 67


def layer_kernel(
    outer_hbm, inner_hbm, input_hbm, taps_hbm, weight_hbm, residual_hbm, ids_hbm, group_hbm, route_hbm,
    gate_hbm, up_hbm, down_hbm, gain_hbm, moe_hbm,
    out_hbm,
    outer_ref, inner_ref, input_ref, taps_ref, weight_ref, residual_ref, ids_ref, group_ref, route_ref, gain_ref, moe_ref,
    halo, sent, got, weights, both, down, tokens, near, far, near_side, far_in, far_side, columns,
    residual_sc, own_acc, line_out, line_in, pair_out, pair_in, hold, back_out, back_in, hidden_sc, final,
    send_sem, recv_sem, local_sem,
):
    sp, tp = lax.axis_index("sp"), lax.axis_index("tp")
    sp_size, tp_size = lax.axis_size("sp"), lax.axis_size("tp")
    core_me, line_me = tp % 2, (tp // 2) % 2
    core_bit = 1 - 2 * core_me
    line_bit = 2 - 4 * line_me
    lanes = [tp, tp + core_bit, tp + line_bit, tp + line_bit + core_bit]
    core, line = (sp, lanes[1]), (sp, lanes[2])
    x_peer = (sp + 1 - 2 * (sp % 2), tp)
    z_peer = (sp + 2 - 4 * ((sp // 2) % 2), tp)
    cross = ((sp + sp_size // 2) % sp_size, tp)
    after, before = ((sp + 1) % sp_size, tp), ((sp + sp_size - 1) % sp_size, tp)
    peers = [core, line, (sp, lanes[3]), x_peer, z_peer, cross]
    first_block, last_block = sp == 0, sp == sp_size - 1

    barrier = pltpu.get_barrier_semaphore()
    for peer in peers:
        pl.semaphore_signal(barrier, inc=1, device_id=peer, device_id_type=MESH)
    for absent, peer in ((last_block, after), (first_block, before)):
        @pl.when(jnp.logical_not(absent))
        def _():
            pl.semaphore_signal(barrier, inc=1, device_id=peer, device_id_type=MESH)

    units = down.shape[2]
    slots, cuts = down.shape[0], down.shape[1]
    fetched = []
    for cut in range(cuts):
        first = pl.multiple_of((tp ^ cut) * units, units)
        fetched += [
            pltpu.make_async_copy(gate_hbm.at[0, :, pl.ds(first, units)], both.at[0, cut, :, pl.ds(0, units)], local_sem.at[3 * cut]),
            pltpu.make_async_copy(up_hbm.at[0, :, pl.ds(first, units)], both.at[0, cut, :, pl.ds(units, units)], local_sem.at[3 * cut + 1]),
            pltpu.make_async_copy(down_hbm.at[0, pl.ds(first, units), :], down.at[0, cut], local_sem.at[3 * cut + 2]),
        ]
    for copy in fetched[:3]:
        copy.start()
    sources = dict(
        ids=(ids_hbm, ids_ref), group=(group_hbm, group_ref), route=(route_hbm, route_ref), inner=(inner_hbm, inner_ref),
        input=(input_hbm, input_ref), outer=(outer_hbm, outer_ref), taps=(taps_hbm, taps_ref), weight=(weight_hbm, weight_ref),
        gain=(gain_hbm, gain_ref), moe=(moe_hbm, moe_ref), residual=(residual_hbm, residual_ref),
    )
    loaded = {}
    for number, name in enumerate(sources):
        loaded[name] = pltpu.make_async_copy(*sources[name], local_sem.at[3 * cuts + number])
        loaded[name].start()
    pl.semaphore_wait(barrier, jnp.where(first_block | last_block, len(peers) + 1, len(peers) + 2))

    started = []

    def prepare(source, target, peer):
        number = len(started)
        copy = pltpu.make_async_remote_copy(
            src_ref=source, dst_ref=target, send_sem=send_sem.at[number], recv_sem=recv_sem.at[number],
            device_id=peer, device_id_type=MESH,
        )
        started.append(copy)
        return copy

    def send(source, target, peer):
        copy = prepare(source, target, peer)
        copy.start()
        return copy

    full = inner_ref.shape[0]
    rows, width = residual_ref.shape
    ends = (sp < 2) | (sp >= sp_size - 2)
    middle = jnp.logical_not(ends)
    halos = [
        prepare(inner_hbm.at[pl.ds(full - HALO_ROWS, HALO_ROWS)], halo.at[0], after),
        prepare(input_hbm.at[pl.ds(full - HALO_ROWS, HALO_ROWS)], halo.at[1], after),
    ]

    def only(where, action, *arguments):
        @pl.when(where)
        def _():
            for argument in arguments:
                action(argument)

    only(jnp.logical_not(last_block), lambda copy: copy.start(), *halos)
    strips = 4
    strip = weight_ref.shape[0] // (2 * strips)
    x_me = sp % 2

    def weight_rows(side, number):
        return pl.ds(pl.multiple_of((strips * side + number) * strip, strip), strip)

    weight_line = [
        send(weight_hbm.at[weight_rows(x_me, number)], weights.at[1, weight_rows(x_me, number)], line) for number in range(strips)
    ]
    weight_core = send(weight_hbm, weights.at[0], core)
    deep, wide = width // 4, units // 4

    def slices(slot, cut):
        return [both.at[slot, cut, pl.ds(n * deep, deep)] for n in range(4)] + [
            down.at[slot, cut, pl.ds(n * wide, wide)] for n in range(4)
        ]

    z_part = [prepare(source, target, z_peer) for source, target in zip(slices(0, 0), slices(1, 0))]
    for copy in fetched[:2]:
        copy.wait()
    z_part[0].start()
    for name in ("ids", "group", "route"):
        loaded[name].wait()
    ids = ids_ref[...]
    route = route_ref[...]
    scale = group_ref[...] * route / jnp.sum(route, axis=0, keepdims=True)
    half = sp_size // 2
    for number, flip in enumerate((0, 2, 1, 3)):
        side = (sp % half) ^ flip
        for table, base in ((near, (sp // half) * half), (far, (1 - sp // half) * half)):
            chosen = jnp.where(ids == base + side, scale, 0.0)
            table[number : number + 1, :] = jnp.sum(chosen, axis=0, keepdims=True)
    far_copy = send(far, far_in, cross)
    near_copy = send(near, near_side, x_peer)
    for copy in z_part[1:4]:
        copy.start()
    fetched[2].wait()
    only(middle, lambda number: z_part[number].start(), 4, 5, 6, 7)
    for copy in fetched[3:]:
        copy.start()
    z_core, z_line, z_both = [], [], []

    def beyond(cut, target, number, sends):
        pair = pl.ds((number // 2) * 2 * deep, 2 * deep)
        if number in (1, 3):
            sends.append(send(both.at[1, cut, pair], both.at[1, target, pair], core))
        if number == 7:
            sends.append(send(down.at[1, cut], down.at[1, target], core))

    def z_arrived(number):
        z_part[number].wait_recv()
        z_line.append(send(slices(1, 0)[number], slices(1, 2)[number], line))
        beyond(0, 1, number, z_core)

    def line_arrived(number):
        z_line[number].wait_recv()
        beyond(2, 3, number, z_both)

    for name in ("inner", "input", "outer", "taps", "gain", "moe"):
        loaded[name].wait()

    only(jnp.logical_not(first_block), lambda copy: copy.wait_recv(), *halos)
    taps = taps_ref[...].astype(jnp.float32)
    count = taps.shape[0]
    exchanged = []
    for step in (2, 3, 1, 0):
        block = lanes[step]
        first = pl.multiple_of(block * rows, rows)
        inner = inner_ref[pl.ds(first, rows)].astype(jnp.float32) * input_ref[pl.ds(first, rows)].astype(jnp.float32)
        back = pl.multiple_of(jnp.maximum(block * rows - HALO_ROWS, 0), HALO_ROWS)
        behind = inner_ref[pl.ds(back, HALO_ROWS)].astype(jnp.float32) * input_ref[pl.ds(back, HALO_ROWS)].astype(jnp.float32)
        outside = halo[0].astype(jnp.float32) * halo[1].astype(jnp.float32)
        outside = jnp.where(sp == 0, 0.0, outside)
        behind = jnp.where(block == 0, outside, behind)
        padded = jnp.concatenate([behind, inner], axis=0)
        filtered = jnp.zeros_like(inner)
        for offset in range(count):
            start = HALO_ROWS - (count - 1) + offset
            filtered = filtered + taps[offset][None, :] * padded[start : start + rows]
        mixed = (outer_ref[pl.ds(first, rows)].astype(jnp.float32) * filtered).astype(jnp.bfloat16)
        sent[step, :rows] = mixed
        sent[step, rows:] = jnp.broadcast_to(gain_ref[...].reshape(1, -1), (GAIN_ROWS, mixed.shape[1]))
        if step > 0:
            exchanged.append(send(sent.at[step], got.at[step - 1], (sp, block)))

    piece = rows // PARTS
    batch = 2 * piece
    blocks = [sent.at[0], got.at[0], got.at[1], got.at[2]]
    matrices = [weight_ref, weights.at[0], weights.at[1], weights.at[2]]

    def gained(block, take):
        gain = block[rows:][:1].astype(jnp.float32)
        return (block[take].astype(jnp.float32) * gain).astype(jnp.bfloat16)

    def squares(block):
        values = block[:rows].astype(jnp.float32)
        return jnp.sum(values * values, axis=1, keepdims=True)

    def product(number, take):
        return jnp.dot(gained(blocks[number], take), matrices[number][...], preferred_element_type=jnp.float32)

    exchanged[2].wait_recv()
    weight_core.wait_recv()
    loaded["weight"].wait()
    loaded["residual"].wait()
    for number in range(2):
        take = slice(number * batch, (number + 1) * batch)
        own_acc[number] = product(0, take) + product(1, take)
    partial = squares(blocks[0]) + squares(blocks[1])

    weight_x, weight_both = [], []

    def weight_pair(side, number):
        if number % 2 == 1:
            rows_at = pl.ds(pl.multiple_of((strips * side + number - 1) * strip, 2 * strip), 2 * strip)
            weight_both.append(send(weights.at[1, rows_at], weights.at[2, rows_at], core))

    for number in range(strips):
        weight_line[number].wait_recv()
        arrived = weights.at[1, weight_rows(x_me, number)]
        weight_x.append(send(arrived, arrived, x_peer))
        weight_pair(x_me, number)
    z_arrived(0)
    z_arrived(1)
    for number in range(strips):
        weight_x[number].wait_recv()
        weight_pair(1 - x_me, number)
    far_copy.wait_recv()
    far_relay = send(far_in, far_side, x_peer)
    near_copy.wait_recv()
    for copy in exchanged[:2]:
        copy.wait_recv()
    total = partial + squares(blocks[2]) + squares(blocks[3])
    factor = lax.rsqrt(total / (tp_size * inner_ref.shape[1]) + EPSILON)
    for copy in weight_both:
        copy.wait_recv()
    own_at, line_at, pair_at = (4, 5), (2, 3), (0, 1, 6, 7)
    def own_rows(part):
        return tokens.at[own_at[part // 2], pl.ds((part % 2) * piece, piece)]

    def line_rows(part):
        return tokens.at[line_at[part // 2], pl.ds((part % 2) * piece, piece)]

    def pair_rows(part, second):
        return tokens.at[pair_at[part], pl.ds(second * piece, piece)]

    across, shared = [], []
    for number, unit in enumerate(own_at):
        take = slice(number * batch, (number + 1) * batch)
        projected = own_acc[number] + product(2, take) + product(3, take)
        out = residual_ref[take].astype(jnp.float32) + factor[take] * projected
        residual = out.astype(jnp.bfloat16)
        residual_sc[take] = residual
        floats = residual.astype(jnp.float32)
        mean = jnp.mean(floats * floats, axis=1, keepdims=True)
        routed = floats * lax.rsqrt(mean + EPSILON) * moe_ref[...].reshape(1, -1).astype(jnp.float32)
        tokens[unit] = routed.astype(jnp.bfloat16)
        for part in (2 * number, 2 * number + 1):
            across.append(send(own_rows(part), pair_rows(part, 0), cross))
            shared.append(send(own_rows(part), line_rows(part), x_peer))
        if number == 0:
            only(ends, lambda number: z_part[number].start(), 4, 5, 6, 7)

    beside = [prepare(pair_rows(part, 0), pair_rows(part, 1), x_peer) for part in range(PARTS)]

    def relay(part):
        across[part].wait_recv()
        beside[part].start()

    z_arrived(2)
    line_arrived(0)
    z_arrived(3)
    line_arrived(1)
    only(middle, relay, 0, 1)
    z_arrived(4)
    z_arrived(5)
    line_arrived(2)
    only(ends, relay, 0, 1)
    far_relay.wait_recv()
    for slot in range(slots):
        for unit, table, row in ((own_at, near, slot), (line_at, near_side, slots + slot)):
            column = table[row : row + 1, :].T
            for number in range(2):
                columns[slot, unit[number]] = column[number * batch : (number + 1) * batch]
        here, there = far_in[slot : slot + 1, :].T, far_side[slots + slot : slots + slot + 1, :].T
        for part in range(PARTS):
            take = slice(part * piece, (part + 1) * piece)
            columns[slot, pair_at[part], :piece] = here[take]
            columns[slot, pair_at[part], piece:] = there[take]
    z_arrived(6)
    z_arrived(7)
    line_arrived(3)
    for number in range(4, 8):
        line_arrived(number)
    for copy in fetched[3:]:
        copy.wait()
    for copy in z_core + z_both:
        copy.wait_recv()

    def expert_sum(unit, store):
        rows_in = tokens[unit]
        for slot in range(slots):
            scale_in = columns[slot, unit]
            for cut in range(cuts):
                act = jnp.dot(rows_in, both[slot, cut], preferred_element_type=jnp.float32)
                gated = jax.nn.silu(act[:, :units]) * act[:, units:]
                start = (slot * cuts + cut) * units
                hidden_sc[:, start : start + units] = (scale_in * gated).astype(jnp.bfloat16)
        hidden = hidden_sc[...]
        step = width // 4
        for tile in range(4):
            columns_at = pl.ds(tile * step, step)
            matrix = down[:, :, :, tile * step : (tile + 1) * step].reshape(slots * cuts * units, step)
            store(columns_at, jnp.dot(hidden, matrix, preferred_element_type=jnp.float32))

    pairs, lines, returned = [], [], []

    def pair_step(part):
        beside[part].wait_recv()

        def store(columns_at, value):
            hold[part, :, columns_at] = value[:piece]
            pair_out[part, :, columns_at] = value[piece:].astype(jnp.bfloat16)

        expert_sum(pair_at[part], store)
        pairs.append(send(pair_out.at[part], pair_in.at[part], x_peer))

    def return_step(part):
        pairs[part].wait_recv()
        back_out[part] = (hold[part] + pair_in[part].astype(jnp.float32)).astype(jnp.bfloat16)
        returned.append(send(back_out.at[part], back_in.at[part], cross))

    def line_step(number):
        for part in (2 * number, 2 * number + 1):
            shared[part].wait_recv()

        def store(columns_at, value):
            for inside in range(2):
                line_out[2 * number + inside, :, columns_at] = value[inside * piece : (inside + 1) * piece].astype(jnp.bfloat16)

        expert_sum(line_at[number], store)
        for part in (2 * number, 2 * number + 1):
            lines.append(send(line_out.at[part], line_in.at[part], x_peer))

    def own_step(number):
        def store(columns_at, value):
            own_acc[number, :, columns_at] = value

        expert_sum(own_at[number], store)

    pair_step(0)
    only(middle, relay, 2)
    pair_step(1)
    only(middle, relay, 3)
    own_step(0)
    only(ends, relay, 2, 3)
    return_step(0)
    return_step(1)
    pair_step(2)
    own_step(1)
    pair_step(3)
    return_step(2)
    line_step(0)
    return_step(3)
    line_step(1)
    late = pairs + lines + returned + halos
    only(jnp.logical_not(last_block), lambda copy: copy.wait_send(), *halos)
    for copy in started:
        if all(copy is not other for other in late):
            copy.wait_send()
    written = []
    for part in range(PARTS):
        returned[part].wait_recv()
        lines[part].wait_recv()
        inside = pl.ds((part % 2) * piece, piece)
        take = pl.ds(part * piece, piece)
        value = own_acc[part // 2, inside] + residual_sc[take].astype(jnp.float32)
        value = value + line_in[part].astype(jnp.float32) + back_in[part].astype(jnp.float32)
        final[part] = value.astype(jnp.bfloat16)
        written.append(pltpu.make_async_copy(final.at[part], out_hbm.at[take], local_sem.at[part]))
        written[part].start()
    for copy in pairs + lines + returned:
        copy.wait_send()
    for copy in written:
        copy.wait()


def half_slice(
    residual_in,
    gate_outer,
    gate_inner,
    conv_input,
    conv_taps,
    norm_gain,
    out_weight,
    moe_gain,
    expert_ids,
    group_prob,
    route_prob,
    expert_gate,
    expert_up,
    expert_down,
):
    sp, tp = lax.axis_size("sp"), lax.axis_size("tp")
    rows, width = residual_in.shape
    channels = gate_outer.shape[1]
    slots, cuts = 2, tp
    units = expert_gate.shape[2] // tp
    piece = rows // PARTS
    wide = slots * cuts * units
    hbm = pl.BlockSpec(memory_space=pltpu.HBM)
    half = lambda *shape: pltpu.VMEM(shape, jnp.bfloat16)
    single = lambda *shape: pltpu.VMEM(shape, jnp.float32)
    return pl.pallas_call(
        layer_kernel,
        in_specs=[hbm] * 14,
        out_specs=hbm,
        out_shape=jax.ShapeDtypeStruct((rows, width), jnp.bfloat16),
        scratch_shapes=[
            half(*gate_outer.shape),
            half(*gate_inner.shape),
            half(*conv_input.shape),
            half(*conv_taps.shape),
            half(*out_weight.shape),
            half(*residual_in.shape),
            pltpu.VMEM(expert_ids.shape[::-1], jnp.int32),
            single(1, rows),
            single(*route_prob.shape[::-1]),
            half(*norm_gain.shape),
            half(*moe_gain.shape),
            half(2, HALO_ROWS, channels),
            half(tp, rows + GAIN_ROWS, channels),
            half(tp - 1, rows + GAIN_ROWS, channels),
            half(tp - 1, *out_weight.shape),
            half(slots, cuts, width, 2 * units),
            half(slots, cuts, units, width),
            half(8, 2 * piece, width),
            single(2 * slots, rows),
            single(2 * slots, rows),
            single(2 * slots, rows),
            single(2 * slots, rows),
            single(2 * slots, rows),
            single(slots, 8, 2 * piece, 1),
            half(rows, width),
            single(2, 2 * piece, width),
            half(PARTS, piece, width),
            half(PARTS, piece, width),
            half(PARTS, piece, width),
            half(PARTS, piece, width),
            single(PARTS, piece, width),
            half(PARTS, piece, width),
            half(PARTS, piece, width),
            half(2 * piece, wide),
            half(PARTS, piece, width),
            pltpu.SemaphoreType.DMA((COPIES,)),
            pltpu.SemaphoreType.DMA((COPIES,)),
            pltpu.SemaphoreType.DMA((11 + 3 * cuts,)),
        ],
        compiler_params=pltpu.CompilerParams(
            collective_id=0, has_side_effects=True, vmem_limit_bytes=58 * 2**20
        ),
    )(
        gate_outer, gate_inner, conv_input, conv_taps, out_weight, residual_in, expert_ids.T, group_prob[None],
        route_prob.T, expert_gate, expert_up, expert_down, norm_gain, moe_gain,
    )


def exchange_slots(
    residual_in,
    gate_outer,
    gate_inner,
    conv_input,
    conv_taps,
    norm_gain,
    out_weight,
    moe_gain,
    expert_ids,
    group_prob,
    route_prob,
    expert_gate,
    expert_up,
    expert_down,
):
    seq_rows, channels = conv_input.shape
    taps_count = conv_taps.shape[0]
    inner = gate_inner.astype(jnp.float32) * conv_input.astype(jnp.float32)
    earlier = from_behind(inner[seq_rows - (taps_count - 1) :], "sp", 1)
    padded = jnp.concatenate([earlier, inner], axis=0)
    tap_f = conv_taps.astype(jnp.float32)
    filtered = jnp.zeros((seq_rows, channels), jnp.float32)
    for offset in range(taps_count):
        filtered = filtered + tap_f[offset][None, :] * padded[offset : offset + seq_rows]
    mixed_out = (gate_outer.astype(jnp.float32) * filtered).astype(jnp.bfloat16)
    gathered = lax.all_to_all(mixed_out, "tp", split_axis=0, concat_axis=1, tiled=True)
    full_weight, full_gain = (
        lax.all_gather(out_weight, "tp", axis=0, tiled=True),
        lax.all_gather(norm_gain, "tp", axis=0, tiled=True),
    )
    normed = rms_norm(gathered, full_gain).astype(jnp.bfloat16)
    projected = jnp.dot(normed, full_weight, preferred_element_type=jnp.float32)
    residual = (residual_in.astype(jnp.float32) + projected).astype(jnp.bfloat16)
    routed_in = rms_norm(residual, moe_gain).astype(jnp.bfloat16)
    tok_rows, width = routed_in.shape
    top_count = expert_ids.shape[1]
    local_count = expert_gate.shape[0]
    group_count = lax.axis_size("sp")
    experts_all = local_count * group_count
    capacity = 2 * tok_rows * top_count // experts_all
    slots = tok_rows * top_count
    flat_e = expert_ids.reshape(-1)
    one_hot = (flat_e[:, None] == jnp.arange(experts_all, dtype=jnp.int32)[None, :]).astype(
        jnp.int32
    )
    slot_rank = jnp.sum((jnp.cumsum(one_hot, axis=0) - 1) * one_hot, axis=1)
    owner_dev = flat_e // local_count
    local_slot = flat_e % local_count
    position = (local_slot * group_count + owner_dev) * capacity + slot_rank
    source_slot = (
        jnp.full((experts_all * capacity,), slots, jnp.int32)
        .at[position]
        .set(jnp.arange(slots, dtype=jnp.int32))
    )
    rows_pad = jnp.concatenate([routed_in, jnp.zeros((1, width), jnp.bfloat16)], axis=0)
    outgoing = rows_pad[source_slot // top_count].reshape(local_count, group_count, capacity, width)
    arrived = lax.all_to_all(outgoing, "sp", split_axis=1, concat_axis=1, tiled=True)
    gate_act = jnp.einsum(
        "esrd,edf->esrf", arrived, expert_gate, preferred_element_type=jnp.float32
    )
    up_act = jnp.einsum("esrd,edf->esrf", arrived, expert_up, preferred_element_type=jnp.float32)
    hidden = (jax.nn.silu(gate_act) * up_act).astype(jnp.bfloat16)
    result = jnp.einsum(
        "esrf,efd->esrd", hidden, expert_down, preferred_element_type=jnp.float32
    ).astype(jnp.bfloat16)
    returned = lax.all_to_all(result, "sp", split_axis=1, concat_axis=1, tiled=True)
    slot_out = returned.reshape(-1, width)[position].reshape(tok_rows, top_count, width)
    weights = group_prob[:, None] * route_prob / jnp.sum(route_prob, axis=1, keepdims=True)
    expert_sum = jnp.sum(slot_out.astype(jnp.float32) * weights[:, :, None], axis=1)
    return (residual.astype(jnp.float32) + expert_sum).astype(jnp.bfloat16)


def solution(mesh):
    in_specs = (
        P(("sp", "tp"), None),
        P("sp", "tp"),
        P("sp", "tp"),
        P("sp", "tp"),
        P(None, "tp"),
        P("tp"),
        P("tp", None),
        P(),
        P(("sp", "tp"), None),
        P(("sp", "tp")),
        P(("sp", "tp"), None),
        P("sp", None, None),
        P("sp", None, None),
        P("sp", None, None),
    )
    out_specs = P(("sp", "tp"), None)
    sp, tp = mesh.shape["sp"], mesh.shape["tp"]

    def body(*args):
        gate, outer = args[11], args[1]
        gathered = 3 * gate.size * gate.dtype.itemsize * sp // 4
        pairs = gate.shape[0] == 1 and sp == 8 and tp == 4
        sized = gate.shape[2] == 128 * tp and outer.shape[0] % (256 * tp) == 0
        if pairs and sized and gathered <= GATHER_BYTES:
            return half_slice(*args)
        return exchange_slots(*args)

    return jax.shard_map(body, mesh=mesh, in_specs=in_specs, out_specs=out_specs, check_vma=False)
```

```python
import jax
import jax.numpy as jnp
from jax import lax
from jax.experimental import pallas as pl
from jax.experimental.pallas import tpu as pltpu
from jax.sharding import PartitionSpec as P

MESH = pl.DeviceIdType.MESH
EPSILON = 1e-06


def from_behind(shard, axis, by):
    devices = lax.axis_size(axis)
    pairs = [(i, i + by) for i in range(devices) if 0 <= i + by < devices]
    return lax.ppermute(shard, axis, pairs)


def rms_norm(values, gain):
    floats = values.astype(jnp.float32)
    factor = lax.rsqrt(jnp.mean(floats * floats, axis=-1, keepdims=True) + EPSILON)
    return floats * factor * gain.astype(jnp.float32)


GATHER_BYTES = 26 * 2**20
GAIN_ROWS = 16
HALO_ROWS = 16
PARTS = 4
COPIES = 69


def layer_kernel(
    outer_hbm, inner_hbm, input_hbm, taps_hbm, weight_hbm, residual_hbm, ids_hbm, group_hbm, route_hbm,
    gate_hbm, up_hbm, down_hbm, gain_hbm, moe_hbm,
    out_hbm,
    outer_ref, inner_ref, input_ref, taps_ref, weight_ref, residual_ref, ids_ref, group_ref, route_ref, gain_ref, moe_ref,
    halo, sent, got, weights, both, down, tokens, near, far, near_side, far_in, far_side, columns,
    residual_sc, own_acc, line_out, line_in, pair_out, pair_in, hold, back_out, back_in, hidden_sc, final,
    send_sem, recv_sem, local_sem,
):
    sp, tp = lax.axis_index("sp"), lax.axis_index("tp")
    sp_size, tp_size = lax.axis_size("sp"), lax.axis_size("tp")
    core_me, line_me = tp % 2, (tp // 2) % 2
    core_bit = 1 - 2 * core_me
    line_bit = 2 - 4 * line_me
    lanes = [tp, tp + core_bit, tp + line_bit, tp + line_bit + core_bit]
    core, line = (sp, lanes[1]), (sp, lanes[2])
    x_peer = (sp + 1 - 2 * (sp % 2), tp)
    z_peer = (sp + 2 - 4 * ((sp // 2) % 2), tp)
    cross = ((sp + sp_size // 2) % sp_size, tp)
    after, before = ((sp + 1) % sp_size, tp), ((sp + sp_size - 1) % sp_size, tp)
    peers = [core, line, (sp, lanes[3]), x_peer, z_peer, cross]
    first_block, last_block = sp == 0, sp == sp_size - 1

    barrier = pltpu.get_barrier_semaphore()
    for peer in peers:
        pl.semaphore_signal(barrier, inc=1, device_id=peer, device_id_type=MESH)
    for absent, peer in ((last_block, after), (first_block, before)):
        @pl.when(jnp.logical_not(absent))
        def _():
            pl.semaphore_signal(barrier, inc=1, device_id=peer, device_id_type=MESH)

    units = down.shape[2]
    slots, cuts = down.shape[0], down.shape[1]
    fetched = []
    for cut in range(cuts):
        first = pl.multiple_of((tp ^ cut) * units, units)
        fetched += [
            pltpu.make_async_copy(gate_hbm.at[0, :, pl.ds(first, units)], both.at[0, cut, :, pl.ds(0, units)], local_sem.at[3 * cut]),
            pltpu.make_async_copy(up_hbm.at[0, :, pl.ds(first, units)], both.at[0, cut, :, pl.ds(units, units)], local_sem.at[3 * cut + 1]),
            pltpu.make_async_copy(down_hbm.at[0, pl.ds(first, units), :], down.at[0, cut], local_sem.at[3 * cut + 2]),
        ]
    for copy in fetched[:3]:
        copy.start()
    sources = dict(
        ids=(ids_hbm, ids_ref), group=(group_hbm, group_ref), route=(route_hbm, route_ref), inner=(inner_hbm, inner_ref),
        input=(input_hbm, input_ref), outer=(outer_hbm, outer_ref), taps=(taps_hbm, taps_ref), weight=(weight_hbm, weight_ref),
        gain=(gain_hbm, gain_ref), moe=(moe_hbm, moe_ref), residual=(residual_hbm, residual_ref),
    )
    loaded = {}
    for number, name in enumerate(sources):
        loaded[name] = pltpu.make_async_copy(*sources[name], local_sem.at[3 * cuts + number])
        loaded[name].start()
    pl.semaphore_wait(barrier, jnp.where(first_block | last_block, len(peers) + 1, len(peers) + 2))

    started = []

    def prepare(source, target, peer):
        number = len(started)
        copy = pltpu.make_async_remote_copy(
            src_ref=source, dst_ref=target, send_sem=send_sem.at[number], recv_sem=recv_sem.at[number],
            device_id=peer, device_id_type=MESH,
        )
        started.append(copy)
        return copy

    def send(source, target, peer):
        copy = prepare(source, target, peer)
        copy.start()
        return copy

    full = inner_ref.shape[0]
    rows, width = residual_ref.shape
    ends = (sp < 2) | (sp >= sp_size - 2)
    middle = jnp.logical_not(ends)
    halos = [
        prepare(inner_hbm.at[pl.ds(full - HALO_ROWS, HALO_ROWS)], halo.at[0], after),
        prepare(input_hbm.at[pl.ds(full - HALO_ROWS, HALO_ROWS)], halo.at[1], after),
    ]

    def only(where, action, *arguments):
        @pl.when(where)
        def _():
            for argument in arguments:
                action(argument)

    only(jnp.logical_not(last_block), lambda copy: copy.start(), *halos)
    strips = 4
    strip = weight_ref.shape[0] // (2 * strips)
    x_me = sp % 2

    def weight_rows(side, number):
        return pl.ds(pl.multiple_of((strips * side + number) * strip, strip), strip)

    weight_line = [
        send(weight_hbm.at[weight_rows(x_me, number)], weights.at[1, weight_rows(x_me, number)], line) for number in range(strips)
    ]
    weight_core = send(weight_hbm, weights.at[0], core)
    deep, wide = width // 4, units // 4

    def slices(slot, cut):
        return [both.at[slot, cut, pl.ds(n * deep, deep)] for n in range(4)] + [
            down.at[slot, cut, pl.ds(n * wide, wide)] for n in range(4)
        ]

    z_part = [prepare(source, target, z_peer) for source, target in zip(slices(0, 0), slices(1, 0))]
    for copy in fetched[:2]:
        copy.wait()
    z_part[0].start()
    for name in ("ids", "group", "route"):
        loaded[name].wait()
    ids = ids_ref[...]
    route = route_ref[...]
    scale = group_ref[...] * route / jnp.sum(route, axis=0, keepdims=True)
    half = sp_size // 2
    for number, flip in enumerate((0, 2, 1, 3)):
        side = (sp % half) ^ flip
        for table, base in ((near, (sp // half) * half), (far, (1 - sp // half) * half)):
            chosen = jnp.where(ids == base + side, scale, 0.0)
            table[number : number + 1, :] = jnp.sum(chosen, axis=0, keepdims=True)
    far_copy = send(far, far_in, cross)
    near_copy = send(near, near_side, x_peer)
    for copy in z_part[1:4]:
        copy.start()
    fetched[2].wait()
    only(middle, lambda number: z_part[number].start(), 4, 5, 6, 7)
    for copy in fetched[3:]:
        copy.start()
    z_core, z_line, z_both = [], [], []

    def beyond(cut, target, number, sends):
        pair = pl.ds((number // 2) * 2 * deep, 2 * deep)
        if number in (1, 3):
            sends.append(send(both.at[1, cut, pair], both.at[1, target, pair], core))
        if number in (5, 7):
            some = pl.ds((number - 5) * wide, 2 * wide)
            sends.append(send(down.at[1, cut, some], down.at[1, target, some], core))

    def z_arrived(number):
        z_part[number].wait_recv()
        z_line.append(send(slices(1, 0)[number], slices(1, 2)[number], line))
        beyond(0, 1, number, z_core)

    def line_arrived(number):
        z_line[number].wait_recv()
        beyond(2, 3, number, z_both)

    for name in ("inner", "input", "outer", "taps", "gain", "moe"):
        loaded[name].wait()

    only(jnp.logical_not(first_block), lambda copy: copy.wait_recv(), *halos)
    taps = taps_ref[...].astype(jnp.float32)
    count = taps.shape[0]
    exchanged = []
    for step in (2, 3, 1, 0):
        block = lanes[step]
        first = pl.multiple_of(block * rows, rows)
        inner = inner_ref[pl.ds(first, rows)].astype(jnp.float32) * input_ref[pl.ds(first, rows)].astype(jnp.float32)
        back = pl.multiple_of(jnp.maximum(block * rows - HALO_ROWS, 0), HALO_ROWS)
        behind = inner_ref[pl.ds(back, HALO_ROWS)].astype(jnp.float32) * input_ref[pl.ds(back, HALO_ROWS)].astype(jnp.float32)
        outside = halo[0].astype(jnp.float32) * halo[1].astype(jnp.float32)
        outside = jnp.where(sp == 0, 0.0, outside)
        behind = jnp.where(block == 0, outside, behind)
        padded = jnp.concatenate([behind, inner], axis=0)
        filtered = jnp.zeros_like(inner)
        for offset in range(count):
            start = HALO_ROWS - (count - 1) + offset
            filtered = filtered + taps[offset][None, :] * padded[start : start + rows]
        mixed = (outer_ref[pl.ds(first, rows)].astype(jnp.float32) * filtered).astype(jnp.bfloat16)
        sent[step, :rows] = mixed
        sent[step, rows:] = jnp.broadcast_to(gain_ref[...].reshape(1, -1), (GAIN_ROWS, mixed.shape[1]))
        if step > 0:
            exchanged.append(send(sent.at[step], got.at[step - 1], (sp, block)))

    piece = rows // PARTS
    batch = 2 * piece
    blocks = [sent.at[0], got.at[0], got.at[1], got.at[2]]
    matrices = [weight_ref, weights.at[0], weights.at[1], weights.at[2]]

    def gained(block, take):
        gain = block[rows:][:1].astype(jnp.float32)
        return (block[take].astype(jnp.float32) * gain).astype(jnp.bfloat16)

    def squares(block):
        values = block[:rows].astype(jnp.float32)
        return jnp.sum(values * values, axis=1, keepdims=True)

    def product(number, take):
        return jnp.dot(gained(blocks[number], take), matrices[number][...], preferred_element_type=jnp.float32)

    exchanged[2].wait_recv()
    weight_core.wait_recv()
    loaded["weight"].wait()
    loaded["residual"].wait()
    for number in range(2):
        take = slice(number * batch, (number + 1) * batch)
        own_acc[number] = product(0, take) + product(1, take)
    partial = squares(blocks[0]) + squares(blocks[1])

    weight_x, weight_both = [], []

    def weight_pair(side, number):
        if number % 2 == 1:
            rows_at = pl.ds(pl.multiple_of((strips * side + number - 1) * strip, 2 * strip), 2 * strip)
            weight_both.append(send(weights.at[1, rows_at], weights.at[2, rows_at], core))

    for number in range(strips):
        weight_line[number].wait_recv()
        arrived = weights.at[1, weight_rows(x_me, number)]
        weight_x.append(send(arrived, arrived, x_peer))
        weight_pair(x_me, number)
    z_arrived(0)
    z_arrived(1)
    for number in range(strips):
        weight_x[number].wait_recv()
        weight_pair(1 - x_me, number)
    far_copy.wait_recv()
    far_relay = send(far_in, far_side, x_peer)
    near_copy.wait_recv()
    for copy in exchanged[:2]:
        copy.wait_recv()
    total = partial + squares(blocks[2]) + squares(blocks[3])
    factor = lax.rsqrt(total / (tp_size * inner_ref.shape[1]) + EPSILON)
    for copy in weight_both:
        copy.wait_recv()
    own_at, line_at, pair_at = (4, 5), (2, 3), (0, 1, 6, 7)
    def own_rows(part):
        return tokens.at[own_at[part // 2], pl.ds((part % 2) * piece, piece)]

    def line_rows(part):
        return tokens.at[line_at[part // 2], pl.ds((part % 2) * piece, piece)]

    def pair_rows(part, second):
        return tokens.at[pair_at[part], pl.ds(second * piece, piece)]

    across, shared = [], []
    for number, unit in enumerate(own_at):
        take = slice(number * batch, (number + 1) * batch)
        projected = own_acc[number] + product(2, take) + product(3, take)
        out = residual_ref[take].astype(jnp.float32) + factor[take] * projected
        residual = out.astype(jnp.bfloat16)
        residual_sc[take] = residual
        floats = residual.astype(jnp.float32)
        mean = jnp.mean(floats * floats, axis=1, keepdims=True)
        routed = floats * lax.rsqrt(mean + EPSILON) * moe_ref[...].reshape(1, -1).astype(jnp.float32)
        tokens[unit] = routed.astype(jnp.bfloat16)
        for part in (2 * number, 2 * number + 1):
            across.append(send(own_rows(part), pair_rows(part, 0), cross))
            shared.append(send(own_rows(part), line_rows(part), x_peer))
        if number == 0:
            only(ends, lambda number: z_part[number].start(), 4, 5, 6, 7)

    beside = [prepare(pair_rows(part, 0), pair_rows(part, 1), x_peer) for part in range(PARTS)]

    def relay(part):
        across[part].wait_recv()
        beside[part].start()

    z_arrived(2)
    line_arrived(0)
    z_arrived(3)
    line_arrived(1)
    only(middle, relay, 0, 1)
    z_arrived(4)
    z_arrived(5)
    line_arrived(2)
    only(ends, relay, 0, 1)
    far_relay.wait_recv()
    for slot in range(slots):
        for unit, table, row in ((own_at, near, slot), (line_at, near_side, slots + slot)):
            column = table[row : row + 1, :].T
            for number in range(2):
                columns[slot, unit[number]] = column[number * batch : (number + 1) * batch]
        here, there = far_in[slot : slot + 1, :].T, far_side[slots + slot : slots + slot + 1, :].T
        for part in range(PARTS):
            take = slice(part * piece, (part + 1) * piece)
            columns[slot, pair_at[part], :piece] = here[take]
            columns[slot, pair_at[part], piece:] = there[take]
    z_arrived(6)
    z_arrived(7)
    for number in range(3, 7):
        line_arrived(number)
    for copy in fetched[3:]:
        copy.wait()
    for copy in z_core[:2] + z_both[:2]:
        copy.wait_recv()

    def expert_hidden(unit):
        rows_in = tokens[unit]
        for slot in range(slots):
            scale_in = columns[slot, unit]
            for cut in range(cuts):
                act = jnp.dot(rows_in, both[slot, cut], preferred_element_type=jnp.float32)
                gated = jax.nn.silu(act[:, :units]) * act[:, units:]
                start = (slot * cuts + cut) * units
                hidden_sc[:, start : start + units] = (scale_in * gated).astype(jnp.bfloat16)

    def expert_down(store):
        hidden = hidden_sc[...]
        step = width // 4
        for tile in range(4):
            columns_at = pl.ds(tile * step, step)
            matrix = down[:, :, :, tile * step : (tile + 1) * step].reshape(slots * cuts * units, step)
            store(columns_at, jnp.dot(hidden, matrix, preferred_element_type=jnp.float32))

    def expert_sum(unit, store):
        expert_hidden(unit)
        expert_down(store)

    pairs, lines, returned = [], [], []

    def pair_step(part):
        beside[part].wait_recv()

        def store(columns_at, value):
            hold[part, :, columns_at] = value[:piece]
            pair_out[part, :, columns_at] = value[piece:].astype(jnp.bfloat16)

        if part == 0:
            expert_hidden(pair_at[0])
            line_arrived(7)
            for copy in z_core[2:] + z_both[2:]:
                copy.wait_recv()
            expert_down(store)
        else:
            expert_sum(pair_at[part], store)
        pairs.append(send(pair_out.at[part], pair_in.at[part], x_peer))

    def return_step(part):
        pairs[part].wait_recv()
        back_out[part] = (hold[part] + pair_in[part].astype(jnp.float32)).astype(jnp.bfloat16)
        returned.append(send(back_out.at[part], back_in.at[part], cross))

    def line_step(number):
        for part in (2 * number, 2 * number + 1):
            shared[part].wait_recv()

        def store(columns_at, value):
            for inside in range(2):
                line_out[2 * number + inside, :, columns_at] = value[inside * piece : (inside + 1) * piece].astype(jnp.bfloat16)

        expert_sum(line_at[number], store)
        for part in (2 * number, 2 * number + 1):
            lines.append(send(line_out.at[part], line_in.at[part], x_peer))

    def own_step(number):
        def store(columns_at, value):
            own_acc[number, :, columns_at] = value

        expert_sum(own_at[number], store)

    pair_step(0)
    only(middle, relay, 2)
    pair_step(1)
    only(middle, relay, 3)
    own_step(0)
    only(ends, relay, 2, 3)
    return_step(0)
    return_step(1)
    pair_step(2)
    own_step(1)
    pair_step(3)
    line_step(0)
    return_step(2)
    line_step(1)
    return_step(3)
    late = pairs + lines + returned + halos
    only(jnp.logical_not(last_block), lambda copy: copy.wait_send(), *halos)
    for copy in started:
        if all(copy is not other for other in late):
            copy.wait_send()
    written = []
    for part in range(PARTS):
        returned[part].wait_recv()
        lines[part].wait_recv()
        inside = pl.ds((part % 2) * piece, piece)
        take = pl.ds(part * piece, piece)
        value = own_acc[part // 2, inside] + residual_sc[take].astype(jnp.float32)
        value = value + line_in[part].astype(jnp.float32) + back_in[part].astype(jnp.float32)
        final[part] = value.astype(jnp.bfloat16)
        written.append(pltpu.make_async_copy(final.at[part], out_hbm.at[take], local_sem.at[part]))
        written[part].start()
    for copy in pairs + lines + returned:
        copy.wait_send()
    for copy in written:
        copy.wait()


def half_slice(
    residual_in,
    gate_outer,
    gate_inner,
    conv_input,
    conv_taps,
    norm_gain,
    out_weight,
    moe_gain,
    expert_ids,
    group_prob,
    route_prob,
    expert_gate,
    expert_up,
    expert_down,
):
    sp, tp = lax.axis_size("sp"), lax.axis_size("tp")
    rows, width = residual_in.shape
    channels = gate_outer.shape[1]
    slots, cuts = 2, tp
    units = expert_gate.shape[2] // tp
    piece = rows // PARTS
    wide = slots * cuts * units
    hbm = pl.BlockSpec(memory_space=pltpu.HBM)
    half = lambda *shape: pltpu.VMEM(shape, jnp.bfloat16)
    single = lambda *shape: pltpu.VMEM(shape, jnp.float32)
    return pl.pallas_call(
        layer_kernel,
        in_specs=[hbm] * 14,
        out_specs=hbm,
        out_shape=jax.ShapeDtypeStruct((rows, width), jnp.bfloat16),
        scratch_shapes=[
            half(*gate_outer.shape),
            half(*gate_inner.shape),
            half(*conv_input.shape),
            half(*conv_taps.shape),
            half(*out_weight.shape),
            half(*residual_in.shape),
            pltpu.VMEM(expert_ids.shape[::-1], jnp.int32),
            single(1, rows),
            single(*route_prob.shape[::-1]),
            half(*norm_gain.shape),
            half(*moe_gain.shape),
            half(2, HALO_ROWS, channels),
            half(tp, rows + GAIN_ROWS, channels),
            half(tp - 1, rows + GAIN_ROWS, channels),
            half(tp - 1, *out_weight.shape),
            half(slots, cuts, width, 2 * units),
            half(slots, cuts, units, width),
            half(8, 2 * piece, width),
            single(2 * slots, rows),
            single(2 * slots, rows),
            single(2 * slots, rows),
            single(2 * slots, rows),
            single(2 * slots, rows),
            single(slots, 8, 2 * piece, 1),
            half(rows, width),
            single(2, 2 * piece, width),
            half(PARTS, piece, width),
            half(PARTS, piece, width),
            half(PARTS, piece, width),
            half(PARTS, piece, width),
            single(PARTS, piece, width),
            half(PARTS, piece, width),
            half(PARTS, piece, width),
            half(2 * piece, wide),
            half(PARTS, piece, width),
            pltpu.SemaphoreType.DMA((COPIES,)),
            pltpu.SemaphoreType.DMA((COPIES,)),
            pltpu.SemaphoreType.DMA((11 + 3 * cuts,)),
        ],
        compiler_params=pltpu.CompilerParams(
            collective_id=0, has_side_effects=True, vmem_limit_bytes=58 * 2**20
        ),
    )(
        gate_outer, gate_inner, conv_input, conv_taps, out_weight, residual_in, expert_ids.T, group_prob[None],
        route_prob.T, expert_gate, expert_up, expert_down, norm_gain, moe_gain,
    )


def exchange_slots(
    residual_in,
    gate_outer,
    gate_inner,
    conv_input,
    conv_taps,
    norm_gain,
    out_weight,
    moe_gain,
    expert_ids,
    group_prob,
    route_prob,
    expert_gate,
    expert_up,
    expert_down,
):
    seq_rows, channels = conv_input.shape
    taps_count = conv_taps.shape[0]
    inner = gate_inner.astype(jnp.float32) * conv_input.astype(jnp.float32)
    earlier = from_behind(inner[seq_rows - (taps_count - 1) :], "sp", 1)
    padded = jnp.concatenate([earlier, inner], axis=0)
    tap_f = conv_taps.astype(jnp.float32)
    filtered = jnp.zeros((seq_rows, channels), jnp.float32)
    for offset in range(taps_count):
        filtered = filtered + tap_f[offset][None, :] * padded[offset : offset + seq_rows]
    mixed_out = (gate_outer.astype(jnp.float32) * filtered).astype(jnp.bfloat16)
    gathered = lax.all_to_all(mixed_out, "tp", split_axis=0, concat_axis=1, tiled=True)
    full_weight, full_gain = (
        lax.all_gather(out_weight, "tp", axis=0, tiled=True),
        lax.all_gather(norm_gain, "tp", axis=0, tiled=True),
    )
    normed = rms_norm(gathered, full_gain).astype(jnp.bfloat16)
    projected = jnp.dot(normed, full_weight, preferred_element_type=jnp.float32)
    residual = (residual_in.astype(jnp.float32) + projected).astype(jnp.bfloat16)
    routed_in = rms_norm(residual, moe_gain).astype(jnp.bfloat16)
    tok_rows, width = routed_in.shape
    top_count = expert_ids.shape[1]
    local_count = expert_gate.shape[0]
    group_count = lax.axis_size("sp")
    experts_all = local_count * group_count
    capacity = 2 * tok_rows * top_count // experts_all
    slots = tok_rows * top_count
    flat_e = expert_ids.reshape(-1)
    one_hot = (flat_e[:, None] == jnp.arange(experts_all, dtype=jnp.int32)[None, :]).astype(
        jnp.int32
    )
    slot_rank = jnp.sum((jnp.cumsum(one_hot, axis=0) - 1) * one_hot, axis=1)
    owner_dev = flat_e // local_count
    local_slot = flat_e % local_count
    position = (local_slot * group_count + owner_dev) * capacity + slot_rank
    source_slot = (
        jnp.full((experts_all * capacity,), slots, jnp.int32)
        .at[position]
        .set(jnp.arange(slots, dtype=jnp.int32))
    )
    rows_pad = jnp.concatenate([routed_in, jnp.zeros((1, width), jnp.bfloat16)], axis=0)
    outgoing = rows_pad[source_slot // top_count].reshape(local_count, group_count, capacity, width)
    arrived = lax.all_to_all(outgoing, "sp", split_axis=1, concat_axis=1, tiled=True)
    gate_act = jnp.einsum(
        "esrd,edf->esrf", arrived, expert_gate, preferred_element_type=jnp.float32
    )
    up_act = jnp.einsum("esrd,edf->esrf", arrived, expert_up, preferred_element_type=jnp.float32)
    hidden = (jax.nn.silu(gate_act) * up_act).astype(jnp.bfloat16)
    result = jnp.einsum(
        "esrf,efd->esrd", hidden, expert_down, preferred_element_type=jnp.float32
    ).astype(jnp.bfloat16)
    returned = lax.all_to_all(result, "sp", split_axis=1, concat_axis=1, tiled=True)
    slot_out = returned.reshape(-1, width)[position].reshape(tok_rows, top_count, width)
    weights = group_prob[:, None] * route_prob / jnp.sum(route_prob, axis=1, keepdims=True)
    expert_sum = jnp.sum(slot_out.astype(jnp.float32) * weights[:, :, None], axis=1)
    return (residual.astype(jnp.float32) + expert_sum).astype(jnp.bfloat16)


def solution(mesh):
    in_specs = (
        P(("sp", "tp"), None),
        P("sp", "tp"),
        P("sp", "tp"),
        P("sp", "tp"),
        P(None, "tp"),
        P("tp"),
        P("tp", None),
        P(),
        P(("sp", "tp"), None),
        P(("sp", "tp")),
        P(("sp", "tp"), None),
        P("sp", None, None),
        P("sp", None, None),
        P("sp", None, None),
    )
    out_specs = P(("sp", "tp"), None)
    sp, tp = mesh.shape["sp"], mesh.shape["tp"]

    def body(*args):
        gate, outer = args[11], args[1]
        gathered = 3 * gate.size * gate.dtype.itemsize * sp // 4
        pairs = gate.shape[0] == 1 and sp == 8 and tp == 4
        sized = gate.shape[2] == 128 * tp and outer.shape[0] % (256 * tp) == 0
        if pairs and sized and gathered <= GATHER_BYTES:
            return half_slice(*args)
        return exchange_slots(*args)

    return jax.shard_map(body, mesh=mesh, in_specs=in_specs, out_specs=out_specs, check_vma=False)
```
